512 devices in a mesh: fs: 64 (over z, y), tp: 8 (over x, core).
Axes of the slice: x: 4, y: 4, z: 16, core: 2. Of those that a mesh axis runs over, the one named last changes fastest.
Arguments:
- saved_inputs: bfloat16 [49152, 2048], P('fs'), may hold values from -16 to 16
- input_cot: bfloat16 [49152, 2048], P('fs', 'tp'), may hold values from -0.02734375 to 0.02734375
- gate_cot: bfloat16 [49152, 2048], P('fs', 'tp'), may hold values from -0.02734375 to 0.02734375
- input_master: float32 [2048, 2048], P('fs', 'tp'), may hold values from -6 to 6
- gate_master: float32 [2048, 2048], P('fs', 'tp'), may hold values from -6 to 6
- input_factor: bfloat16 [2048, 256], P('fs'), may hold values from -2 to 2
- gate_factor: bfloat16 [2048, 256], P('fs'), may hold values from -2 to 2
- input_first: float32 [256, 2048], P('fs', 'tp'), may hold values from -6 to 6
- input_second: float32 [256, 2048], P('fs', 'tp'), may hold values from 0.2 to 17
- gate_first: float32 [256, 2048], P('fs', 'tp'), may hold values from -6 to 6
- gate_second: float32 [256, 2048], P('fs', 'tp'), may hold values from 0.2 to 17
Outputs:
- input_step: float32 [2048, 2048], P('fs', 'tp')
- gate_step: float32 [2048, 2048], P('fs', 'tp')
- input_first_new: float32 [256, 2048], P('fs', 'tp')
- input_second_new: float32 [256, 2048], P('fs', 'tp')
- gate_first_new: float32 [256, 2048], P('fs', 'tp')
- gate_second_new: float32 [256, 2048], P('fs', 'tp')
- input_copy: bfloat16 [2048, 2048], P(None, 'tp')
- gate_copy: bfloat16 [2048, 2048], P(None, 'tp')
The draws below stay inside these ranges and needn't reach their ends.
All inputs are finite; a program needn't handle non-finite values.
Results may differ from the reference program's by a relative error of at most 0.0004.
Values may be sent and summed in bfloat16 or wider, within the bound.
A program may use at most 64 MiB of HBM per device.

```python
import jax
import jax.numpy as jnp
from jax import lax

D = 2048
W = 2048
RANK = 256
TOKENS = 49152


def factor_draw(key, salt):
    keyed = jax.random.fold_in(key, salt)
    key_one, key_two = jax.random.split(keyed)
    position = jnp.arange(D, dtype=jnp.float32)[:, None] / D
    jitter = jnp.exp(jax.random.uniform(key_one, (D, 1), jnp.float32, -0.7, 0.7))
    scales = jnp.exp(jnp.log(6.0) * position) * jitter / 2.8
    entries = jax.random.normal(key_two, (D, RANK), jnp.float32)
    values = jnp.clip(entries * scales * D ** (-0.5), -2.0, 2.0)
    return values.astype(jnp.bfloat16)


def second_draw(key, salt):
    keyed = jax.random.fold_in(key, salt)
    column = jnp.arange(W, dtype=jnp.float32)[None, :] / W
    jitter = jnp.exp(jax.random.uniform(keyed, (RANK, W), jnp.float32, -0.7, 0.7))
    spread = jnp.exp(jnp.log(9.0) * (1.0 - column))
    return (0.5 * jitter * spread).astype(jnp.float32)


def draw_input_factor(key, part):
    return factor_draw(key, 11)


def draw_gate_factor(key, part):
    return factor_draw(key, 23)


def draw_input_second(key, part):
    return second_draw(key, 37)


def draw_gate_second(key, part):
    return second_draw(key, 41)


def raised(result, key, source, target, shards_of, factor):
    owner, partner = [(jnp.arange(result.shape[axis_at]) // (result.shape[axis_at] // shards_of)).reshape([-1 if axis == axis_at else 1 for axis in range(result.ndim)]) for axis_at in (source, target)]
    chosen = jax.random.permutation(key, shards_of)[partner]
    strong = (owner == chosen) | (owner == (partner + shards_of // 2) % shards_of)
    return jnp.where(strong, factor * result, result)


def block_levels(own_key, shape, shards, smallest, high):
    loudness = 1.0
    for axis_at, parts in shards:
        heights = jax.random.uniform(jax.random.fold_in(jax.random.fold_in(own_key, 6), axis_at), (parts,), jnp.float32, smallest / len(shards), high / len(shards))
        loudness = loudness * jnp.repeat(jnp.exp(heights), shape[axis_at] // parts).reshape((-1,) + (1,) * (len(shape) - 1 - axis_at))
    return loudness


def gaussian(own_key, shape, scale, most, cuts=(), kind=jnp.bfloat16):
    values = scale * jax.random.normal(own_key, shape, jnp.float32)
    if cuts:
        values = values * block_levels(own_key, shape, cuts, -0.22, 0.18)
    return jnp.clip(values, -most, most).astype(kind)


def gaussian_with(own_key, dims, deviation, reach, shards, heavy, kind=jnp.bfloat16):
    values = deviation * jax.random.normal(own_key, dims, jnp.float32)
    if shards:
        values = values * block_levels(own_key, dims, shards, -0.22, 0.18)
    return jnp.clip(raised(values, jax.random.fold_in(own_key, 3), *heavy), -reach, reach).astype(kind)


def setup_inputs(seed: int = 0) -> dict:
    key_of = jax.random.split(jax.random.key(seed), 12)
    saved_inputs = gaussian_with(key_of[0], (TOKENS, D), 1.0, 16.0, ((0, 64),), (0, 1, 64, 4.0))
    input_cot = gaussian(key_of[1], (TOKENS, W), (TOKENS ** -0.5), 0.02734375, ((0, 64), (1, 8)))
    gate_cot = gaussian(key_of[2], (TOKENS, W), (TOKENS ** -0.5), 0.02734375, ((0, 64), (1, 8)))
    input_master = gaussian(key_of[3], (D, W), 1.0, 6.0, ((0, 64), (1, 8)), jnp.float32)
    gate_master = gaussian(key_of[4], (D, W), 1.0, 6.0, ((0, 64), (1, 8)), jnp.float32)
    input_factor = draw_input_factor(jax.random.fold_in(key_of[11], 71), 0)
    gate_factor = draw_gate_factor(jax.random.fold_in(key_of[11], 71), 0)
    input_first = gaussian(key_of[7], (RANK, W), 1.0, 6.0, ((0, 64), (1, 8)), jnp.float32)
    input_second = draw_input_second(jax.random.fold_in(key_of[11], 71), 0)
    gate_first = gaussian(key_of[9], (RANK, W), 1.0, 6.0, ((0, 64), (1, 8)), jnp.float32)
    gate_second = draw_gate_second(jax.random.fold_in(key_of[11], 71), 0)
    return {"saved_inputs": saved_inputs, "input_cot": input_cot, "gate_cot": gate_cot, "input_master": input_master, "gate_master": gate_master, "input_factor": input_factor, "gate_factor": gate_factor, "input_first": input_first, "input_second": input_second, "gate_first": gate_first, "gate_second": gate_second}


first_decay = 0.9
second_decay = 0.9
ratio_floor = 1e-08
mean_floor = 1e-06
step_size = 0.05

def update_one(saved_inputs, cotangent, master, factor, first, second):
    contract = (((0,), (0,)), ((), ()))
    gradient = lax.dot_general(saved_inputs, cotangent, contract, preferred_element_type=jnp.float32)
    factor_wide = factor.astype(jnp.float32)
    low_rank = lax.dot_general(factor_wide, gradient, contract, precision=lax.Precision.HIGHEST)
    first_new = first_decay * first + (1.0 - first_decay) * low_rank
    second_new = second_decay * second + (1.0 - second_decay) * low_rank * low_rank
    ratio = first_new / (jnp.sqrt(second_new) + ratio_floor)
    direction = jnp.dot(factor_wide, ratio, precision=lax.Precision.HIGHEST)
    step = direction * lax.rsqrt(jnp.mean(direction * direction) + mean_floor)
    weights_copy = (master - step_size * step).astype(jnp.bfloat16)
    return (step, first_new, second_new, weights_copy)

def reference(saved_inputs, input_cot, gate_cot, input_master, gate_master, input_factor, gate_factor, input_first, input_second, gate_first, gate_second):
    step_in, first_in, second_in, copy_in = update_one(saved_inputs, input_cot, input_master, input_factor, input_first, input_second)
    step_gate, first_gate, second_gate, copy_gate = update_one(saved_inputs, gate_cot, gate_master, gate_factor, gate_first, gate_second)
    return (step_in, step_gate, first_in, second_in, first_gate, second_gate, copy_in, copy_gate)
```

```python
import functools

import jax
import jax.numpy as jnp
from jax import lax
from jax.experimental import pallas as pl
from jax.experimental.pallas import tpu as pltpu
from jax.sharding import Mesh
from jax.sharding import PartitionSpec as P

D = 2048
W = 2048
FS = ("fs_0", "fs_1")
TP = ("tp_0", "tp_1")
NZ, NY, NX, NC = 16, 4, 4, 2
HALF = NZ // 2

first_decay = 0.9
second_decay = 0.9
ratio_floor = 1e-08
mean_floor = 1e-06
step_size = 0.05

f32 = jnp.float32
bf16 = jnp.bfloat16


def remote(src, dst, send_sem, recv_sem, **where):
    return pltpu.make_async_remote_copy(
        src_ref=src,
        dst_ref=dst,
        send_sem=send_sem,
        recv_sem=recv_sem,
        device_id=where,
        device_id_type=pl.DeviceIdType.MESH,
    )


def split_two(v):
    high = v.astype(bf16)
    low = (v - high.astype(f32)).astype(bf16)
    return high, low


def kernel(
    x_hbm, cin_hbm, cg_hbm, min_hbm, mg_hbm, fin_hbm, fg_hbm, a1, a2, g1, g2,
    step_in, step_g, o_a1, o_a2, o_g1, o_g2, copy_in, copy_g,
    xb, cb, mb, fb, lowb, rsy, l2, rsz, rb, dirb, sb, cpy,
    loc_sem, fz_s, fz_r, f1_s, f1_r, f2_s, f2_r, fc_s, fc_r,
    ry_s, ry_r, rz_s, rz_r, gz_s, gz_r, gy_s, gy_r, sc_s, sc_r,
    cz_s, cz_r, cy_s, cy_r, out_sem,
):
    z = lax.axis_index("fs_0")
    y = lax.axis_index("fs_1")
    x = lax.axis_index("tp_0")
    c = lax.axis_index("tp_1")
    other = 1 - c

    def zz(k):
        return lax.rem(z + k + NZ, NZ)

    def yy(k):
        return lax.rem(y + k + NY, NY)

    def xx(k):
        return lax.rem(x + k + NX, NX)

    barrier = pltpu.get_barrier_semaphore()

    def greet(k, _):
        pl.semaphore_signal(barrier, inc=1, device_id={"fs_0": zz(k)}, device_id_type=pl.DeviceIdType.MESH)
        return 0

    lax.fori_loop(1, NZ, greet, 0)
    for k in range(1, NY):
        pl.semaphore_signal(barrier, inc=1, device_id={"fs_1": yy(k)}, device_id_type=pl.DeviceIdType.MESH)
    tp_peers = [(dx, dc) for dx in range(NX) for dc in range(NC) if (dx, dc) != (0, 0)]
    for dx, dc in tp_peers:
        pl.semaphore_signal(
            barrier, inc=1,
            device_id={"tp_0": xx(dx), "tp_1": other if dc else c},
            device_id_type=pl.DeviceIdType.MESH,
        )

    h = x // 2
    tile = pl.ds(pl.multiple_of((c * 2 + lax.rem(x, 2)) * 128, 128), 128)
    wide = pl.ds(pl.multiple_of(c * 256, 256), 256)
    piece = pl.ds(pl.multiple_of(lax.rem(x, 2) * 128, 128), 128)

    def own_tile(source):
        return pltpu.make_async_copy(source.at[h, :, piece], fb.at[z, y, h, :, tile], loc_sem.at[0])

    @pl.when(c == 0)
    def _():
        own_tile(fin_hbm).start()

    @pl.when(c == 1)
    def _():
        own_tile(fg_hbm).start()

    loads = [
        pltpu.make_async_copy(x_hbm, xb, loc_sem.at[1]),
        pltpu.make_async_copy(cin_hbm, cb.at[0], loc_sem.at[2]),
        pltpu.make_async_copy(cg_hbm, cb.at[1], loc_sem.at[3]),
        pltpu.make_async_copy(min_hbm, mb.at[0], loc_sem.at[4]),
        pltpu.make_async_copy(mg_hbm, mb.at[1], loc_sem.at[5]),
    ]
    for copy in loads:
        copy.start()
    own_tile(fin_hbm).wait()
    pl.semaphore_wait(barrier, NZ - 1 + NY - 1 + len(tp_peers))

    def fz(k):
        part = fb.at[z, y, h, :, tile]
        return remote(part, part, fz_s.at[k], fz_r.at[k], fs_0=zz(k))

    def start(make):
        def body(k, _):
            make(k).start()
            return 0
        return body

    def wait_recv(make):
        def body(k, _):
            make(k).wait_recv()
            return 0
        return body

    def wait_send(make):
        def body(k, _):
            make(k).wait_send()
            return 0
        return body

    lax.fori_loop(1, NZ, start(fz), 0)
    lax.fori_loop(1, NZ, wait_recv(fz), 0)

    def half_step(part_x, part_y, send, recv):
        copies = []
        for k in range(1, NX):
            copies.append(remote(part_x, part_x, send.at[0, k], recv.at[0, k], tp_0=xx(k)))
        for k in range(1, NY):
            copies.append(remote(part_y, part_y, send.at[1, k], recv.at[1, k], fs_1=yy(k)))
        for copy in copies:
            copy.start()
        return copies

    lo_z, hi_z = pl.ds(0, HALF), pl.ds(HALF, HALF)
    one = half_step(fb.at[lo_z, y, h, :, tile], fb.at[hi_z, y, h, :, tile], f1_s, f1_r)
    for copy in one:
        copy.wait_recv()
    two = half_step(fb.at[hi_z, :, h, :, tile], fb.at[lo_z, y, :, :, wide], f2_s, f2_r)
    for copy in two:
        copy.wait_recv()
    mine = fb.at[:, :, :, :, wide]
    swap = remote(mine, mine, fc_s, fc_r, tp_1=other)
    swap.start()
    for copy in loads[:3]:
        copy.wait()
    swap.wait_recv()

    lows = []
    for f in range(2):
        total = jnp.zeros((256, 256), f32)
        factor = fb[:, :, :, :, f * 256:(f + 1) * 256].reshape(D, 256)
        for t in range(3):
            rows = pl.ds(t * 256, 256)
            proj = jnp.dot(xb[rows, :], factor, preferred_element_type=f32)
            high, low = split_two(proj.T)
            cot = cb[f, rows, :]
            total = total + jnp.dot(high, cot, preferred_element_type=f32)
            total = total + jnp.dot(low, cot, preferred_element_type=f32)
        lows.append(total.reshape(32, 8, 256))
    top = lax.broadcasted_iota(jnp.int32, (32, 8, 256), 1) < 4
    low_a, low_b = lows
    even = jnp.where(top, low_a, pltpu.roll(low_b, 4, 1))
    odd = jnp.where(top, pltpu.roll(low_a, 4, 1), low_b)
    for k in range(2):
        lowb[:, 2 * k] = even.reshape(16, 2, 8, 256)[:, k]
        lowb[:, 2 * k + 1] = odd.reshape(16, 2, 8, 256)[:, k]

    ry = [
        remote(lowb.at[:, yy(k)], rsy.at[k - 1], ry_s.at[k], ry_r.at[k], fs_1=yy(k))
        for k in range(1, NY)
    ]
    for copy in ry:
        copy.start()
    acc = lowb[:, y]
    for k, copy in enumerate(ry):
        copy.wait_recv()
        acc = acc + rsy[k]
    l2[...] = acc

    def rz(k):
        return remote(l2.at[zz(k)], rsz.at[k], rz_s.at[k], rz_r.at[k], fs_0=zz(k))

    lax.fori_loop(1, NZ, start(rz), 0)

    def add_one(k, total):
        rz(k).wait_recv()
        return total + rsz[k]

    low = lax.fori_loop(1, NZ, add_one, l2[z])

    first = jnp.concatenate([a1[...], g1[...]], axis=0)
    second = jnp.concatenate([a2[...], g2[...]], axis=0)
    first_new = first_decay * first + (1.0 - first_decay) * low
    second_new = second_decay * second + (1.0 - second_decay) * low * low
    rb[z, y] = first_new / (jnp.sqrt(second_new) + ratio_floor)

    def gz(k):
        part = rb.at[z, y]
        return remote(part, part, gz_s.at[k], gz_r.at[k], fs_0=zz(k))

    lax.fori_loop(1, NZ, start(gz), 0)
    o_a1[...] = first_new[:4]
    o_g1[...] = first_new[4:]
    o_a2[...] = second_new[:4]
    o_g2[...] = second_new[4:]
    lax.fori_loop(1, NZ, wait_recv(gz), 0)
    gy = [
        remote(rb.at[:, y], rb.at[:, y], gy_s.at[k], gy_r.at[k], fs_1=yy(k))
        for k in range(1, NY)
    ]
    for copy in gy:
        copy.start()
    for copy in gy:
        copy.wait_recv()

    ratio = rb[...].reshape(32, 2, 8, 256)
    even, odd = ratio[:, 0], ratio[:, 1]
    pieces = (
        jnp.where(top, even, pltpu.roll(odd, 4, 1)).reshape(256, 256),
        jnp.where(top, pltpu.roll(even, 4, 1), odd).reshape(256, 256),
    )
    for f in range(2):
        high, lo = split_two(pieces[f])

        def rows_of(t, acc, f=f, high=high, lo=lo):
            block = fb[pl.ds(t * 2, 2), :, :, :, f * 256:(f + 1) * 256].reshape(256, 256)
            d = jnp.dot(block, high, preferred_element_type=f32)
            d = d + jnp.dot(block, lo, preferred_element_type=f32)
            dirb[f, pl.ds(pl.multiple_of(t * 256, 256), 256), :] = d
            return acc + jnp.sum((d * d).reshape(32, 8, 256), axis=0)

        acc = lax.fori_loop(0, 8, rows_of, jnp.zeros((8, 256), f32))
        sb[0, f] = acc[:, :128] + acc[:, 128:]

    sc = [
        remote(
            sb.at[0], sb.at[k + 1], sc_s.at[k], sc_r.at[k],
            tp_0=xx(dx), tp_1=other if dc else c,
        )
        for k, (dx, dc) in enumerate(tp_peers)
    ]
    for copy in sc:
        copy.start()
    for copy in loads[3:]:
        copy.wait()
    for copy in sc:
        copy.wait_recv()
    own = pl.ds(pl.multiple_of((z * NY + y) * 32, 32), 32)
    for f, out in enumerate((step_in, step_g)):
        total = jnp.sum(jnp.sum(sb[:, f], axis=0), keepdims=True)
        scale = lax.rsqrt(total / (D * W) + mean_floor)
        step = dirb[f, own, :] * scale
        out[...] = step
        cpy[f, z, y] = (mb[f] - step_size * step).astype(bf16)

    both = pl.ds(0, 2)

    def cz(s, way, mats=both):
        block = cpy.at[mats, zz(1 - s) if way == 0 else zz(s - 1), y]
        return remote(block, block, cz_s.at[way, s], cz_r.at[way, s], fs_0=zz(1 if way == 0 else -1))

    def cy(o, way):
        block = cpy.at[:, zz(o), y]
        return remote(block, block, cy_s.at[way, o], cy_r.at[way, o], fs_1=yy(1 if way == 0 else -1))

    def on(o, way):
        mats = pl.ds(way, 1)
        block = cpy.at[mats, zz(o), yy(-1 if way == 0 else 1)]
        return remote(block, block, cy_s.at[way + 2, o], cy_r.at[way + 2, o], fs_1=yy(1 if way == 0 else -1))

    def send_y(o):
        cy(o, 0).start()
        cy(o, 1).start()

    def pass_y(o):
        cy(o, 0).wait_recv()
        on(o, 0).start()
        cy(o, 1).wait_recv()
        on(o, 1).start()

    cz(1, 0).start()
    cz(1, 1).start()
    send_y(0)

    def ring_one(s, _):
        cz(s, 0).wait_recv()
        cz(s + 1, 0).start()
        cz(s, 1).wait_recv()
        cz(s + 1, 1).start()
        send_y(s)
        send_y(NZ - s)
        return 0

    def ring(s, _):
        ring_one(s, 0)
        pass_y(s - 1)
        pass_y(NZ - s + 1)
        return 0

    ring_one(1, 0)
    pass_y(0)
    lax.fori_loop(2, HALF - 1, ring, 0)
    last = (cz(HALF, 0, pl.ds(0, 1)), cz(HALF, 1, pl.ds(1, 1)))
    for way in range(2):
        cz(HALF - 1, way).wait_recv()
        last[way].start()
    send_y(HALF - 1)
    send_y(HALF + 1)
    pass_y(HALF - 2)
    pass_y(HALF + 2)
    for way in range(2):
        last[way].wait_recv()
    send_y(HALF)
    pass_y(HALF - 1)
    pass_y(HALF + 1)
    pass_y(HALF)

    def finish(o, _):
        on(o, 0).wait_recv()
        on(o, 1).wait_recv()
        return 0

    lax.fori_loop(0, NZ, finish, 0)
    outs = [
        pltpu.make_async_copy(cpy.at[0], copy_in, out_sem.at[0]),
        pltpu.make_async_copy(cpy.at[1], copy_g, out_sem.at[1]),
    ]
    for copy in outs:
        copy.start()

    lax.fori_loop(1, NZ, wait_send(fz), 0)
    lax.fori_loop(1, NZ, wait_send(rz), 0)
    lax.fori_loop(1, NZ, wait_send(gz), 0)
    for copy in [*one, *two, swap, *ry, *gy, *sc, *last]:
        copy.wait_send()

    def drain_z(s, _):
        cz(s, 0).wait_send()
        cz(s, 1).wait_send()
        return 0

    def drain_y(o, _):
        for way in range(2):
            cy(o, way).wait_send()
            on(o, way).wait_send()
        return 0

    lax.fori_loop(1, HALF, drain_z, 0)
    lax.fori_loop(0, NZ, drain_y, 0)
    for copy in outs:
        copy.wait()


def local(x, cin, cg, m_in, m_g, f_in, f_g, a1, a2, g1, g2):
    vmem = pl.BlockSpec(memory_space=pltpu.VMEM)
    hbm = pl.BlockSpec(memory_space=pl.ANY)
    dma = pltpu.SemaphoreType.DMA
    out = pl.pallas_call(
        kernel,
        out_shape=(
            jax.ShapeDtypeStruct((32, 256), f32),
            jax.ShapeDtypeStruct((32, 256), f32),
            jax.ShapeDtypeStruct((4, 256), f32),
            jax.ShapeDtypeStruct((4, 256), f32),
            jax.ShapeDtypeStruct((4, 256), f32),
            jax.ShapeDtypeStruct((4, 256), f32),
            jax.ShapeDtypeStruct((NZ, NY, 32, 256), bf16),
            jax.ShapeDtypeStruct((NZ, NY, 32, 256), bf16),
        ),
        in_specs=[hbm] * 7 + [vmem] * 4,
        out_specs=(vmem,) * 6 + (hbm,) * 2,
        scratch_shapes=[
            pltpu.VMEM((768, 2048), bf16),
            pltpu.VMEM((2, 768, 256), bf16),
            pltpu.VMEM((2, 32, 256), f32),
            pltpu.VMEM((NZ, NY, 2, 16, 512), bf16),
            pltpu.VMEM((NZ, NY, 8, 256), f32),
            pltpu.VMEM((NY - 1, NZ, 8, 256), f32),
            pltpu.VMEM((NZ, 8, 256), f32),
            pltpu.VMEM((NZ, 8, 256), f32),
            pltpu.VMEM((NZ, NY, 8, 256), f32),
            pltpu.VMEM((2, 2048, 256), f32),
            pltpu.VMEM((NX * NC, 2, 8, 128), f32),
            pltpu.VMEM((2, NZ, NY, 32, 256), bf16),
            dma((6,)),
            dma((NZ,)), dma((NZ,)),
            dma((2, 4)), dma((2, 4)), dma((2, 4)), dma((2, 4)),
            dma, dma,
            dma((NY,)), dma((NY,)), dma((NZ,)), dma((NZ,)),
            dma((NZ,)), dma((NZ,)), dma((NY,)), dma((NY,)),
            dma((NX * NC,)), dma((NX * NC,)),
            dma((2, HALF + 1)), dma((2, HALF + 1)),
            dma((4, NZ)), dma((4, NZ)),
            dma((2,)),
        ],
        compiler_params=pltpu.CompilerParams(
            collective_id=0, has_side_effects=True, vmem_limit_bytes=48 * 1024 * 1024
        ),
    )(x, cin, cg, m_in, m_g, f_in.reshape(2, 16, 256), f_g.reshape(2, 16, 256), a1, a2, g1, g2)
    return (*out[:6], out[6].reshape(D, 256), out[7].reshape(D, 256))


def solution(mesh):
    finer = Mesh(mesh.devices.reshape(NZ, NY, NX, NC), ("fs_0", "fs_1", "tp_0", "tp_1"))
    rows, both = P(FS, None), P(FS, TP)
    return jax.shard_map(
        local,
        mesh=finer,
        in_specs=(rows, both, both, both, both, rows, rows, both, both, both, both),
        out_specs=(both,) * 6 + (P(None, TP),) * 2,
        check_vma=False,
    )
```

```python
import functools

import jax
import jax.numpy as jnp
from jax import lax
from jax.experimental import pallas as pl
from jax.experimental.pallas import tpu as pltpu
from jax.sharding import Mesh
from jax.sharding import PartitionSpec as P

D = 2048
W = 2048
FS = ("fs_0", "fs_1")
TP = ("tp_0", "tp_1")
NZ, NY, NX, NC = 16, 4, 4, 2
HALF = NZ // 2

first_decay = 0.9
second_decay = 0.9
ratio_floor = 1e-08
mean_floor = 1e-06
step_size = 0.05

f32 = jnp.float32
bf16 = jnp.bfloat16


def remote(src, dst, send_sem, recv_sem, **where):
    return pltpu.make_async_remote_copy(
        src_ref=src,
        dst_ref=dst,
        send_sem=send_sem,
        recv_sem=recv_sem,
        device_id=where,
        device_id_type=pl.DeviceIdType.MESH,
    )


def split_two(v):
    high = v.astype(bf16)
    low = (v - high.astype(f32)).astype(bf16)
    return high, low


def kernel(
    x_hbm, cin_hbm, cg_hbm, min_hbm, mg_hbm, fin_hbm, fg_hbm, a1_hbm, a2_hbm, g1_hbm, g2_hbm,
    step_in, step_g, o_a1, o_a2, o_g1, o_g2, copy_in, copy_g,
    xb, cb, mf, fb, mom, lowt, lowb, rsy, l2, rsz, rb, dirb, sb, cpy,
    loc_sem, fz_s, fz_r, f1_s, f1_r, f2_s, f2_r, fc_s, fc_r,
    ry_s, ry_r, rz_s, rz_r, gz_s, gz_r, gy_s, gy_r, sc_s, sc_r,
    za_s, za_r, zb_s, zb_r, ya_s, ya_r, yb_s, yb_r, out_sem,
):
    z = lax.axis_index("fs_0")
    y = lax.axis_index("fs_1")
    x = lax.axis_index("tp_0")
    c = lax.axis_index("tp_1")
    other = 1 - c

    def zz(k):
        return lax.rem(z + k + NZ, NZ)

    def yy(k):
        return lax.rem(y + k + NY, NY)

    def xx(k):
        return lax.rem(x + k + NX, NX)

    barrier = pltpu.get_barrier_semaphore()

    def greet(k, _):
        pl.semaphore_signal(barrier, inc=1, device_id={"fs_0": zz(k)}, device_id_type=pl.DeviceIdType.MESH)
        return 0

    lax.fori_loop(1, NZ, greet, 0)
    for k in range(1, NY):
        pl.semaphore_signal(barrier, inc=1, device_id={"fs_1": yy(k)}, device_id_type=pl.DeviceIdType.MESH)
    tp_peers = [(dx, dc) for dx in range(NX) for dc in range(NC) if (dx, dc) != (0, 0)]
    for dx, dc in tp_peers:
        pl.semaphore_signal(
            barrier, inc=1,
            device_id={"tp_0": xx(dx), "tp_1": other if dc else c},
            device_id_type=pl.DeviceIdType.MESH,
        )

    h = x // 2
    tile = pl.ds(pl.multiple_of((c * 2 + lax.rem(x, 2)) * 128, 128), 128)
    wide = pl.ds(pl.multiple_of(c * 256, 256), 256)
    piece = pl.ds(pl.multiple_of(lax.rem(x, 2) * 128, 128), 128)

    def own_tile(source):
        return pltpu.make_async_copy(source.at[h, :, piece], fb.at[z, y, h, :, tile], loc_sem.at[0])

    @pl.when(c == 0)
    def _():
        own_tile(fin_hbm).start()

    @pl.when(c == 1)
    def _():
        own_tile(fg_hbm).start()

    loads = [
        pltpu.make_async_copy(min_hbm, mf.at[0, z, y], loc_sem.at[1]),
        pltpu.make_async_copy(mg_hbm, mf.at[1, z, y], loc_sem.at[2]),
        pltpu.make_async_copy(x_hbm, xb, loc_sem.at[3]),
        pltpu.make_async_copy(cin_hbm, cb.at[0], loc_sem.at[4]),
        pltpu.make_async_copy(cg_hbm, cb.at[1], loc_sem.at[5]),
        pltpu.make_async_copy(a1_hbm, mom.at[0], loc_sem.at[6]),
        pltpu.make_async_copy(g1_hbm, mom.at[1], loc_sem.at[7]),
        pltpu.make_async_copy(a2_hbm, mom.at[2], loc_sem.at[8]),
        pltpu.make_async_copy(g2_hbm, mom.at[3], loc_sem.at[9]),
    ]
    for copy in loads:
        copy.start()
    own_tile(fin_hbm).wait()
    for copy in loads[:2]:
        copy.wait()
    pl.semaphore_wait(barrier, NZ - 1 + NY - 1 + len(tp_peers))

    def step_of(s, way):
        return (zz(1 - s), zz(1)) if way == 0 else (zz(s - 1), zz(-1))

    def za(s, way):
        at, to = step_of(s, way)
        part = mf.at[0, at, y, pl.ds(0, 32) if s < HALF else pl.ds(16 * way, 16)]
        return remote(part, part, za_s.at[way, s], za_r.at[way, s], fs_0=to)

    def zb(s, way):
        at, to = step_of(s, way)
        part = mf.at[1, at, pl.ds(0, 4) if s < HALF else pl.ds(2 * way, 2)]
        return remote(part, part, zb_s.at[way, s], zb_r.at[way, s], fs_0=to)

    def ring_start(make):
        for way in range(2):
            make(1, way).start()

    def ring_next(make, s):
        for way in range(2):
            make(s, way).wait_recv()
            if s < HALF:
                make(s + 1, way).start()

    def ya(o, way):
        part = mf.at[0, zz(o), y]
        return remote(part, part, ya_s.at[way, o], ya_r.at[way, o], fs_1=yy(1 if way == 0 else -1))

    def on(o, way):
        part = mf.at[0, zz(o), yy(-1 if way == 0 else 1), pl.ds(16 * way, 16)]
        return remote(part, part, ya_s.at[way + 2, o], ya_r.at[way + 2, o], fs_1=yy(1 if way == 0 else -1))

    def send_y(offsets):
        for o in offsets:
            for way in range(2):
                ya(o, way).start()

    def pass_y(offsets):
        for o in offsets:
            for way in range(2):
                ya(o, way).wait_recv()
                on(o, way).start()

    yb = [
        remote(mf.at[1, z, y], mf.at[1, z, y], yb_s.at[k], yb_r.at[k], fs_1=yy(k))
        for k in range(1, NY)
    ]

    def fz(k):
        part = fb.at[z, y, h, :, tile]
        return remote(part, part, fz_s.at[k], fz_r.at[k], fs_0=zz(k))

    def start(make):
        def body(k, _):
            make(k).start()
            return 0
        return body

    def wait_recv(make):
        def body(k, _):
            make(k).wait_recv()
            return 0
        return body

    def wait_send(make):
        def body(k, _):
            make(k).wait_send()
            return 0
        return body

    lax.fori_loop(1, NZ, start(fz), 0)
    ring_start(za)
    for copy in yb:
        copy.start()
    for copy in yb:
        copy.wait_recv()
    ring_start(zb)
    ring_next(za, 1)
    ring_next(za, 2)
    lax.fori_loop(1, NZ, wait_recv(fz), 0)

    def half_step(part_x, part_y, send, recv):
        copies = []
        for k in range(1, NX):
            copies.append(remote(part_x, part_x, send.at[0, k], recv.at[0, k], tp_0=xx(k)))
        for k in range(1, NY):
            copies.append(remote(part_y, part_y, send.at[1, k], recv.at[1, k], fs_1=yy(k)))
        for copy in copies:
            copy.start()
        return copies

    lo_z, hi_z = pl.ds(0, HALF), pl.ds(HALF, HALF)
    one = half_step(fb.at[lo_z, y, h, :, tile], fb.at[hi_z, y, h, :, tile], f1_s, f1_r)
    ring_next(zb, 1)
    for copy in one:
        copy.wait_recv()
    two = half_step(fb.at[hi_z, :, h, :, tile], fb.at[lo_z, y, :, :, wide], f2_s, f2_r)
    ring_next(za, 3)
    ring_next(zb, 2)
    for copy in two:
        copy.wait_recv()
    mine = fb.at[:, :, :, :, wide]
    swap = remote(mine, mine, fc_s, fc_r, tp_1=other)
    swap.start()
    ring_next(za, 4)
    for copy in loads[2:]:
        copy.wait()

    def project(f):
        total = jnp.zeros((256, 256), f32)
        factor = fb[:, :, :, :, pl.ds(pl.multiple_of(f * 256, 256), 256)].reshape(D, 256)
        for t in range(3):
            rows = pl.ds(t * 256, 256)
            proj = jnp.dot(xb[rows, :], factor, preferred_element_type=f32)
            high, low = split_two(proj.T)
            cot = cb[f, rows, :]
            total = total + jnp.dot(high, cot, preferred_element_type=f32)
            total = total + jnp.dot(low, cot, preferred_element_type=f32)
        lowt[f] = total.reshape(32, 8, 256)

    project(c)
    ring_next(zb, 3)
    ring_next(za, 5)
    swap.wait_recv()
    project(other)
    top = lax.broadcasted_iota(jnp.int32, (32, 8, 256), 1) < 4
    low_a, low_b = lowt[0], lowt[1]
    even = jnp.where(top, low_a, pltpu.roll(low_b, 4, 1))
    odd = jnp.where(top, pltpu.roll(low_a, 4, 1), low_b)
    for k in range(2):
        lowb[:, 2 * k] = even.reshape(16, 2, 8, 256)[:, k]
        lowb[:, 2 * k + 1] = odd.reshape(16, 2, 8, 256)[:, k]

    ry = [
        remote(lowb.at[:, yy(k)], rsy.at[k - 1], ry_s.at[k], ry_r.at[k], fs_1=yy(k))
        for k in range(1, NY)
    ]
    for copy in ry:
        copy.start()
    ring_next(zb, 4)
    ring_next(za, 6)
    acc = lowb[:, y]
    for k, copy in enumerate(ry):
        copy.wait_recv()
        acc = acc + rsy[k]
    l2[...] = acc

    def rz(k):
        return remote(l2.at[zz(k)], rsz.at[k], rz_s.at[k], rz_r.at[k], fs_0=zz(k))

    lax.fori_loop(1, NZ, start(rz), 0)
    early = [0, *(o for s in range(1, HALF - 1) for o in (s, NZ - s))]
    late = [HALF - 1, HALF + 1, HALF]
    send_y(early)
    ring_next(zb, 5)

    def add_one(k, total):
        rz(k).wait_recv()
        return total + rsz[k]

    low = lax.fori_loop(1, NZ, add_one, l2[z])

    first = jnp.concatenate([mom[0], mom[1]], axis=0)
    second = jnp.concatenate([mom[2], mom[3]], axis=0)
    first_new = first_decay * first + (1.0 - first_decay) * low
    second_new = second_decay * second + (1.0 - second_decay) * low * low
    rb[z, y] = first_new / (jnp.sqrt(second_new) + ratio_floor)

    def gz(k):
        part = rb.at[z, y]
        return remote(part, part, gz_s.at[k], gz_r.at[k], fs_0=zz(k))

    lax.fori_loop(1, NZ, start(gz), 0)
    o_a1[...] = first_new[:4]
    o_g1[...] = first_new[4:]
    o_a2[...] = second_new[:4]
    o_g2[...] = second_new[4:]
    pass_y(early)
    ring_next(zb, 6)
    lax.fori_loop(1, NZ, wait_recv(gz), 0)
    gy = [
        remote(rb.at[:, y], rb.at[:, y], gy_s.at[k], gy_r.at[k], fs_1=yy(k))
        for k in range(1, NY)
    ]
    for copy in gy:
        copy.start()
    ring_next(za, 7)
    ring_next(zb, 7)
    for copy in gy:
        copy.wait_recv()
    ring_next(za, HALF)
    send_y(late)

    ratio = rb[...].reshape(32, 2, 8, 256)
    even, odd = ratio[:, 0], ratio[:, 1]
    pieces = (
        jnp.where(top, even, pltpu.roll(odd, 4, 1)).reshape(256, 256),
        jnp.where(top, pltpu.roll(even, 4, 1), odd).reshape(256, 256),
    )
    for f in range(2):
        high, lo = split_two(pieces[f])

        acc = jnp.zeros((8, 256), f32)
        for t in range(4):
            block = fb[4 * t:4 * t + 4, :, :, :, f * 256:(f + 1) * 256].reshape(512, 256)
            d = jnp.dot(block, high, preferred_element_type=f32)
            d = d + jnp.dot(block, lo, preferred_element_type=f32)
            dirb[f, t] = d.reshape(16, 32, 256)
            acc = acc + jnp.sum((d * d).reshape(64, 8, 256), axis=0)
        sb[0, f] = acc[:, :128] + acc[:, 128:]

    sc = [
        remote(
            sb.at[0], sb.at[k + 1], sc_s.at[k], sc_r.at[k],
            tp_0=xx(dx), tp_1=other if dc else c,
        )
        for k, (dx, dc) in enumerate(tp_peers)
    ]
    for copy in sc:
        copy.start()
    pass_y(late)
    ring_next(zb, HALF)
    for o in [*early, *late]:
        for way in range(2):
            on(o, way).wait_recv()
    for copy in sc:
        copy.wait_recv()
    outs = []
    for f, (out, whole) in enumerate(((step_in, copy_in), (step_g, copy_g))):
        total = jnp.sum(jnp.sum(sb[:, f], axis=0), keepdims=True)
        scale = lax.rsqrt(total / (D * W) + mean_floor)
        for t in range(4):
            step = dirb[f, t] * scale.reshape(1, 1, 1)
            weights = mf[f, 4 * t:4 * t + 4].reshape(16, 32, 256)
            cpy[f, t] = (weights - step_size * step).astype(bf16)
            outs.append(pltpu.make_async_copy(cpy.at[f, t], whole.at[t], out_sem.at[f, t]))
            outs[-1].start()
        out[...] = dirb[f, z // 4, lax.rem(z, 4) * NY + y] * scale

    lax.fori_loop(1, NZ, wait_send(fz), 0)
    lax.fori_loop(1, NZ, wait_send(rz), 0)
    lax.fori_loop(1, NZ, wait_send(gz), 0)
    for copy in [*one, *two, swap, *ry, *gy, *sc, *yb]:
        copy.wait_send()
    for way in range(2):
        for s in range(1, HALF + 1):
            za(s, way).wait_send()
            zb(s, way).wait_send()
        for o in range(NZ):
            ya(o, way).wait_send()
            on(o, way).wait_send()
    for copy in outs:
        copy.wait()


def deliver(*refs):
    sem = refs[16]
    copies = [pltpu.make_async_copy(refs[i], refs[8 + i], sem.at[i]) for i in range(8)]
    for copy in copies:
        copy.start()
    for copy in copies:
        copy.wait()


def local(*args):
    vmem = pl.BlockSpec(memory_space=pltpu.VMEM)
    anywhere = pl.BlockSpec(memory_space=pl.ANY)
    dma = pltpu.SemaphoreType.DMA
    args = list(args)
    for k in (5, 6):
        args[k] = args[k].reshape(2, 16, 256)
    shapes = [jax.ShapeDtypeStruct((32, 256), f32)] * 2 + [jax.ShapeDtypeStruct((4, 256), f32)] * 4
    shapes += [jax.ShapeDtypeStruct((4, 16, 32, 256), bf16)] * 2
    out = pl.pallas_call(
        kernel,
        out_shape=tuple(shapes),
        in_specs=[anywhere] * 11,
        out_specs=(vmem,) * 6 + (anywhere,) * 2,
        scratch_shapes=[
            pltpu.VMEM((768, 2048), bf16),
            pltpu.VMEM((2, 768, 256), bf16),
            pltpu.VMEM((2, NZ, NY, 32, 256), f32),
            pltpu.VMEM((NZ, NY, 2, 16, 512), bf16),
            pltpu.VMEM((4, 4, 256), f32),
            pltpu.VMEM((2, 32, 8, 256), f32),
            pltpu.VMEM((NZ, NY, 8, 256), f32),
            pltpu.VMEM((NY - 1, NZ, 8, 256), f32),
            pltpu.VMEM((NZ, 8, 256), f32),
            pltpu.VMEM((NZ, 8, 256), f32),
            pltpu.VMEM((NZ, NY, 8, 256), f32),
            pltpu.VMEM((2, 4, 16, 32, 256), f32),
            pltpu.VMEM((NX * NC, 2, 8, 128), f32),
            pltpu.VMEM((2, 4, 16, 32, 256), bf16),
            dma((10,)),
            dma((NZ,)), dma((NZ,)),
            dma((2, 4)), dma((2, 4)), dma((2, 4)), dma((2, 4)),
            dma, dma,
            dma((NY,)), dma((NY,)), dma((NZ,)), dma((NZ,)),
            dma((NZ,)), dma((NZ,)), dma((NY,)), dma((NY,)),
            dma((NX * NC,)), dma((NX * NC,)),
            dma((2, HALF + 1)), dma((2, HALF + 1)), dma((2, HALF + 1)), dma((2, HALF + 1)),
            dma((4, NZ)), dma((4, NZ)), dma((NY,)), dma((NY,)),
            dma((2, 4)),
        ],
        compiler_params=pltpu.CompilerParams(
            collective_id=0, has_side_effects=True, vmem_limit_bytes=40 * 1024 * 1024
        ),
    )(*[pltpu.with_memory_space_constraint(a, pltpu.HBM) for a in args])
    out = pl.pallas_call(
        deliver,
        out_shape=tuple(shapes),
        in_specs=[anywhere] * 8,
        out_specs=(anywhere,) * 8,
        scratch_shapes=[dma((8,))],
        compiler_params=pltpu.CompilerParams(vmem_limit_bytes=1024 * 1024),
    )(*out)
    return (*out[:6], out[6].reshape(D, 256), out[7].reshape(D, 256))


def solution(mesh):
    finer = Mesh(mesh.devices.reshape(NZ, NY, NX, NC), ("fs_0", "fs_1", "tp_0", "tp_1"))
    rows, both = P(FS, None), P(FS, TP)
    return jax.shard_map(
        local,
        mesh=finer,
        in_specs=(rows, both, both, both, both, rows, rows, both, both, both, both),
        out_specs=(both,) * 6 + (P(None, TP),) * 2,
        check_vma=False,
    )
```

```python
import functools

import jax
import jax.numpy as jnp
from jax import lax
from jax.experimental import pallas as pl
from jax.experimental.pallas import tpu as pltpu
from jax.sharding import Mesh
from jax.sharding import PartitionSpec as P

D = 2048
W = 2048
FS = ("fs_0", "fs_1")
TP = ("tp_0", "tp_1")
NZ, NY, NX, NC = 16, 4, 4, 2
HALF = NZ // 2

first_decay = 0.9
second_decay = 0.9
ratio_floor = 1e-08
mean_floor = 1e-06
step_size = 0.05

f32 = jnp.float32
bf16 = jnp.bfloat16


def remote(src, dst, send_sem, recv_sem, **where):
    return pltpu.make_async_remote_copy(
        src_ref=src,
        dst_ref=dst,
        send_sem=send_sem,
        recv_sem=recv_sem,
        device_id=where,
        device_id_type=pl.DeviceIdType.MESH,
    )


def split_two(v):
    high = v.astype(bf16)
    low = (v - high.astype(f32)).astype(bf16)
    return high, low


def kernel(
    x_hbm, cin_hbm, cg_hbm, min_hbm, mg_hbm, fin_hbm, fg_hbm, a1_hbm, a2_hbm, g1_hbm, g2_hbm,
    step_in, step_g, o_a1, o_a2, o_g1, o_g2, copy_in, copy_g,
    xb, cb, gt, mf, fb, mom, res, lowb, rsy, l2, rsz, rb, dirb, sb, cpy,
    loc_sem, fz_s, fz_r, f1_s, f1_r, f2_s, f2_r, fc_s, fc_r,
    ry_s, ry_r, rz_s, rz_r, gz_s, gz_r, gy_s, gy_r, sc_s, sc_r,
    za_s, za_r, zb_s, zb_r, ya_s, ya_r, yb_s, yb_r, out_sem,
):
    z = lax.axis_index("fs_0")
    y = lax.axis_index("fs_1")
    x = lax.axis_index("tp_0")
    c = lax.axis_index("tp_1")
    other = 1 - c

    def zz(k):
        return lax.rem(z + k + NZ, NZ)

    def yy(k):
        return lax.rem(y + k + NY, NY)

    def xx(k):
        return lax.rem(x + k + NX, NX)

    barrier = pltpu.get_barrier_semaphore()

    def greet(k, _):
        pl.semaphore_signal(barrier, inc=1, device_id={"fs_0": zz(k)}, device_id_type=pl.DeviceIdType.MESH)
        return 0

    lax.fori_loop(1, NZ, greet, 0)
    for k in range(1, NY):
        pl.semaphore_signal(barrier, inc=1, device_id={"fs_1": yy(k)}, device_id_type=pl.DeviceIdType.MESH)
    tp_peers = [(dx, dc) for dx in range(NX) for dc in range(NC) if (dx, dc) != (0, 0)]
    for dx, dc in tp_peers:
        pl.semaphore_signal(
            barrier, inc=1,
            device_id={"tp_0": xx(dx), "tp_1": other if dc else c},
            device_id_type=pl.DeviceIdType.MESH,
        )

    h = x // 2
    tile = pl.ds(pl.multiple_of((c * 2 + lax.rem(x, 2)) * 128, 128), 128)
    wide = pl.ds(pl.multiple_of(c * 256, 256), 256)
    piece = pl.ds(pl.multiple_of(lax.rem(x, 2) * 128, 128), 128)

    def own_tile(source):
        return pltpu.make_async_copy(source.at[h, :, piece], fb.at[z, y, h, :, tile], loc_sem.at[0])

    @pl.when(c == 0)
    def _():
        own_tile(fin_hbm).start()

    @pl.when(c == 1)
    def _():
        own_tile(fg_hbm).start()

    loads = [
        pltpu.make_async_copy(min_hbm, mf.at[0, z, y], loc_sem.at[1]),
        pltpu.make_async_copy(mg_hbm, mf.at[1, z, y], loc_sem.at[2]),
        pltpu.make_async_copy(x_hbm, xb, loc_sem.at[3]),
        pltpu.make_async_copy(cin_hbm, cb.at[0], loc_sem.at[4]),
        pltpu.make_async_copy(cg_hbm, cb.at[1], loc_sem.at[5]),
        pltpu.make_async_copy(a1_hbm, mom.at[0], loc_sem.at[6]),
        pltpu.make_async_copy(g1_hbm, mom.at[1], loc_sem.at[7]),
        pltpu.make_async_copy(a2_hbm, mom.at[2], loc_sem.at[8]),
        pltpu.make_async_copy(g2_hbm, mom.at[3], loc_sem.at[9]),
    ]
    for copy in loads:
        copy.start()
    own_tile(fin_hbm).wait()
    for copy in loads[:2]:
        copy.wait()
    pl.semaphore_wait(barrier, NZ - 1 + NY - 1 + len(tp_peers))

    def step_of(s, way):
        return (zz(1 - s), zz(1)) if way == 0 else (zz(s - 1), zz(-1))

    def za(s, way):
        at, to = step_of(s, way)
        part = mf.at[0, at, y, pl.ds(0, 32) if s < HALF else pl.ds(16 * way, 16)]
        return remote(part, part, za_s.at[way, s], za_r.at[way, s], fs_0=to)

    def zb(s, way):
        at, to = step_of(s, way)
        part = mf.at[1, at, pl.ds(0, 4) if s < HALF else pl.ds(2 * way, 2)]
        return remote(part, part, zb_s.at[way, s], zb_r.at[way, s], fs_0=to)

    def ring_start(make):
        for way in range(2):
            make(1, way).start()

    def ring_next(make, s):
        for way in range(2):
            make(s, way).wait_recv()
            if s < HALF:
                make(s + 1, way).start()

    def ya(o, way):
        part = mf.at[0, zz(o), y]
        return remote(part, part, ya_s.at[way, o], ya_r.at[way, o], fs_1=yy(1 if way == 0 else -1))

    def on(o, way):
        part = mf.at[0, zz(o), yy(-1 if way == 0 else 1), pl.ds(16 * way, 16)]
        return remote(part, part, ya_s.at[way + 2, o], ya_r.at[way + 2, o], fs_1=yy(1 if way == 0 else -1))

    def send_y(offsets):
        for o in offsets:
            for way in range(2):
                ya(o, way).start()

    def pass_y(offsets):
        for o in offsets:
            for way in range(2):
                ya(o, way).wait_recv()
                on(o, way).start()

    yb = [
        remote(mf.at[1, z, y], mf.at[1, z, y], yb_s.at[k], yb_r.at[k], fs_1=yy(k))
        for k in range(1, NY)
    ]

    def fz(k):
        part = fb.at[z, y, h, :, tile]
        return remote(part, part, fz_s.at[k], fz_r.at[k], fs_0=zz(k))

    def start(make):
        def body(k, _):
            make(k).start()
            return 0
        return body

    def wait_recv(make):
        def body(k, _):
            make(k).wait_recv()
            return 0
        return body

    def wait_send(make):
        def body(k, _):
            make(k).wait_send()
            return 0
        return body

    lax.fori_loop(1, NZ, start(fz), 0)
    ring_start(za)
    for copy in yb:
        copy.start()
    for copy in loads[2:]:
        copy.wait()

    def gradient(f):
        cot = cb[f].T
        for t in range(4):
            columns = pl.ds(t * 512, 512)
            high, low = split_two(jnp.dot(cot, xb[:, columns], preferred_element_type=f32))
            gt[f, pl.ds(0, 256), columns] = high
            gt[f, pl.ds(256, 256), columns] = low

    gradient(0)
    for copy in yb:
        copy.wait_recv()
    ring_start(zb)
    ring_next(za, 1)
    gradient(1)
    ring_next(za, 2)
    lax.fori_loop(1, NZ, wait_recv(fz), 0)

    def half_step(part_x, part_y, send, recv):
        copies = []
        for k in range(1, NX):
            copies.append(remote(part_x, part_x, send.at[0, k], recv.at[0, k], tp_0=xx(k)))
        for k in range(1, NY):
            copies.append(remote(part_y, part_y, send.at[1, k], recv.at[1, k], fs_1=yy(k)))
        for copy in copies:
            copy.start()
        return copies

    lo_z, hi_z = pl.ds(0, HALF), pl.ds(HALF, HALF)
    one = half_step(fb.at[lo_z, y, h, :, tile], fb.at[hi_z, y, h, :, tile], f1_s, f1_r)
    ring_next(zb, 1)
    for copy in one:
        copy.wait_recv()
    two = half_step(fb.at[hi_z, :, h, :, tile], fb.at[lo_z, y, :, :, wide], f2_s, f2_r)
    ring_next(za, 3)
    ring_next(zb, 2)
    for copy in two:
        copy.wait_recv()
    mine = fb.at[:, :, :, :, wide]
    swap = remote(mine, mine, fc_s, fc_r, tp_1=other)
    swap.start()
    ring_next(za, 4)
    top = lax.broadcasted_iota(jnp.int32, (32, 8, 128), 1) < 4
    pair = (c, other)

    def project(f):
        factor = fb[:, :, :, :, pl.ds(pl.multiple_of(f * 256, 256), 256)].reshape(D, 256)
        both = jnp.dot(gt[f], factor, preferred_element_type=f32)
        low = (both[:256] + both[256:]).T.reshape(32, 8, 256)
        left, right = low[:, :, :128], low[:, :, 128:]
        even = jnp.where(top, left, pltpu.roll(right, 4, 1)).reshape(16, 2, 8, 128)
        odd = jnp.where(top, pltpu.roll(left, 4, 1), right).reshape(16, 2, 8, 128)
        for k in range(2):
            lowb[f, :, 2 * k] = even[:, k]
            lowb[f, :, 2 * k + 1] = odd[:, k]

    def sum_y(j):
        copies = [
            remote(lowb.at[pair[j], :, yy(k)], rsy.at[j, k - 1], ry_s.at[j, k], ry_r.at[j, k], fs_1=yy(k))
            for k in range(1, NY)
        ]
        for copy in copies:
            copy.start()
        return copies

    def rz(j):
        return lambda k: remote(l2.at[j, zz(k)], rsz.at[j, k], rz_s.at[j, k], rz_r.at[j, k], fs_0=zz(k))

    def gz(j):
        part = rb.at[j, z, y]
        return lambda k: remote(part, part, gz_s.at[j, k], gz_r.at[j, k], fs_0=zz(k))

    project(c)
    ry = [sum_y(0)]
    ring_next(zb, 3)
    ring_next(za, 5)
    swap.wait_recv()
    project(other)
    ry.append(sum_y(1))
    ring_next(zb, 4)
    ring_next(za, 6)
    for j in range(2):
        acc = lowb[pair[j], :, y]
        for k, copy in enumerate(ry[j]):
            copy.wait_recv()
            acc = acc + rsy[j, k]
        l2[j] = acc
        lax.fori_loop(1, NZ, start(rz(j)), 0)
    early = [0, *(o for s in range(1, HALF - 1) for o in (s, NZ - s))]
    late = [HALF - 1, HALF + 1, HALF]
    send_y(early)
    ring_next(zb, 5)

    def folded(v):
        return jnp.concatenate([v[:, :128], v[:, 128:]], axis=0)

    def unfolded(v):
        return jnp.concatenate([v[:4], v[4:]], axis=1)

    for j in range(2):
        def add_one(k, total, j=j):
            rz(j)(k).wait_recv()
            return total + rsz[j, k]

        low = lax.fori_loop(1, NZ, add_one, l2[j, z])
        first_new = first_decay * folded(mom[pair[j]]) + (1.0 - first_decay) * low
        second_new = second_decay * folded(mom[2 + pair[j]]) + (1.0 - second_decay) * low * low
        rb[j, z, y] = first_new / (jnp.sqrt(second_new) + ratio_floor)
        lax.fori_loop(1, NZ, start(gz(j)), 0)
        res[pair[j]] = unfolded(first_new)
        res[2 + pair[j]] = unfolded(second_new)
    pass_y(early)
    ring_next(zb, 6)
    gy = []
    for j in range(2):
        lax.fori_loop(1, NZ, wait_recv(gz(j)), 0)
        part = rb.at[j, :, y]
        gy.append([
            remote(part, part, gy_s.at[j, k], gy_r.at[j, k], fs_1=yy(k)) for k in range(1, NY)
        ])
        for copy in gy[j]:
            copy.start()
    for k, out in enumerate((o_a1, o_g1, o_a2, o_g2)):
        out[...] = res[k]
    ring_next(za, 7)
    ring_next(zb, 7)
    ring_next(za, HALF)
    send_y(late)
    for j in range(2):
        f = pair[j]
        for copy in gy[j]:
            copy.wait_recv()
        ratio = rb[j].reshape(32, 2, 8, 128)
        even, odd = ratio[:, 0], ratio[:, 1]
        left = jnp.where(top, even, pltpu.roll(odd, 4, 1)).reshape(256, 128)
        right = jnp.where(top, pltpu.roll(even, 4, 1), odd).reshape(256, 128)
        high, lo = split_two(jnp.concatenate([left, right], axis=1))
        acc = jnp.zeros((8, 256), f32)
        for t in range(4):
            block = fb[4 * t:4 * t + 4, :, :, :, pl.ds(pl.multiple_of(f * 256, 256), 256)].reshape(512, 256)
            d = jnp.dot(block, high, preferred_element_type=f32)
            d = d + jnp.dot(block, lo, preferred_element_type=f32)
            dirb[f, t] = d.reshape(16, 32, 256)
            acc = acc + jnp.sum((d * d).reshape(64, 8, 256), axis=0)
        sb[0, f] = acc[:, :128] + acc[:, 128:]

    sc = [
        remote(
            sb.at[0], sb.at[k + 1], sc_s.at[k], sc_r.at[k],
            tp_0=xx(dx), tp_1=other if dc else c,
        )
        for k, (dx, dc) in enumerate(tp_peers)
    ]
    for copy in sc:
        copy.start()
    pass_y(late)
    ring_next(zb, HALF)
    for o in [*early, *late]:
        for way in range(2):
            on(o, way).wait_recv()
    for copy in sc:
        copy.wait_recv()
    outs = []
    for f, (out, whole) in enumerate(((step_in, copy_in), (step_g, copy_g))):
        total = jnp.sum(jnp.sum(sb[:, f], axis=0), keepdims=True)
        scale = lax.rsqrt(total / (D * W) + mean_floor)
        for t in range(4):
            step = dirb[f, t] * scale.reshape(1, 1, 1)
            weights = mf[f, 4 * t:4 * t + 4].reshape(16, 32, 256)
            cpy[f, t] = (weights - step_size * step).astype(bf16)
            outs.append(pltpu.make_async_copy(cpy.at[f, t], whole.at[t], out_sem.at[f, t]))
            outs[-1].start()
        out[...] = dirb[f, z // 4, lax.rem(z, 4) * NY + y] * scale

    lax.fori_loop(1, NZ, wait_send(fz), 0)
    for j in range(2):
        lax.fori_loop(1, NZ, wait_send(rz(j)), 0)
        lax.fori_loop(1, NZ, wait_send(gz(j)), 0)
    for copy in [*one, *two, swap, *ry[0], *ry[1], *gy[0], *gy[1], *sc, *yb]:
        copy.wait_send()
    for way in range(2):
        for s in range(1, HALF + 1):
            za(s, way).wait_send()
            zb(s, way).wait_send()
        for o in range(NZ):
            ya(o, way).wait_send()
            on(o, way).wait_send()
    for copy in outs:
        copy.wait()


def deliver(*refs):
    sem = refs[16]
    copies = [pltpu.make_async_copy(refs[i], refs[8 + i], sem.at[i]) for i in range(8)]
    for copy in copies:
        copy.start()
    for copy in copies:
        copy.wait()


def local(*args):
    vmem = pl.BlockSpec(memory_space=pltpu.VMEM)
    anywhere = pl.BlockSpec(memory_space=pl.ANY)
    dma = pltpu.SemaphoreType.DMA
    args = list(args)
    for k in (5, 6):
        args[k] = args[k].reshape(2, 16, 256)
    shapes = [jax.ShapeDtypeStruct((32, 256), f32)] * 2 + [jax.ShapeDtypeStruct((4, 256), f32)] * 4
    shapes += [jax.ShapeDtypeStruct((4, 16, 32, 256), bf16)] * 2
    out = pl.pallas_call(
        kernel,
        out_shape=tuple(shapes),
        in_specs=[anywhere] * 11,
        out_specs=(vmem,) * 6 + (anywhere,) * 2,
        scratch_shapes=[
            pltpu.VMEM((768, 2048), bf16),
            pltpu.VMEM((2, 768, 256), bf16),
            pltpu.VMEM((2, 512, 2048), bf16),
            pltpu.VMEM((2, NZ, NY, 32, 256), f32),
            pltpu.VMEM((NZ, NY, 2, 16, 512), bf16),
            pltpu.VMEM((4, 4, 256), f32),
            pltpu.VMEM((4, 4, 256), f32),
            pltpu.VMEM((2, NZ, NY, 8, 128), f32),
            pltpu.VMEM((2, NY - 1, NZ, 8, 128), f32),
            pltpu.VMEM((2, NZ, 8, 128), f32),
            pltpu.VMEM((2, NZ, 8, 128), f32),
            pltpu.VMEM((2, NZ, NY, 8, 128), f32),
            pltpu.VMEM((2, 4, 16, 32, 256), f32),
            pltpu.VMEM((NX * NC, 2, 8, 128), f32),
            pltpu.VMEM((2, 4, 16, 32, 256), bf16),
            dma((10,)),
            dma((NZ,)), dma((NZ,)),
            dma((2, 4)), dma((2, 4)), dma((2, 4)), dma((2, 4)),
            dma, dma,
            dma((2, NY)), dma((2, NY)), dma((2, NZ)), dma((2, NZ)),
            dma((2, NZ)), dma((2, NZ)), dma((2, NY)), dma((2, NY)),
            dma((NX * NC,)), dma((NX * NC,)),
            dma((2, HALF + 1)), dma((2, HALF + 1)), dma((2, HALF + 1)), dma((2, HALF + 1)),
            dma((4, NZ)), dma((4, NZ)), dma((NY,)), dma((NY,)),
            dma((2, 4)),
        ],
        compiler_params=pltpu.CompilerParams(
            collective_id=0, has_side_effects=True, vmem_limit_bytes=40 * 1024 * 1024
        ),
    )(*[pltpu.with_memory_space_constraint(a, pltpu.HBM) for a in args])
    out = pl.pallas_call(
        deliver,
        out_shape=tuple(shapes),
        in_specs=[anywhere] * 8,
        out_specs=(anywhere,) * 8,
        scratch_shapes=[dma((8,))],
        compiler_params=pltpu.CompilerParams(vmem_limit_bytes=1024 * 1024),
    )(*out)
    return (*out[:6], out[6].reshape(D, 256), out[7].reshape(D, 256))


def solution(mesh):
    finer = Mesh(mesh.devices.reshape(NZ, NY, NX, NC), ("fs_0", "fs_1", "tp_0", "tp_1"))
    rows, both = P(FS, None), P(FS, TP)
    return jax.shard_map(
        local,
        mesh=finer,
        in_specs=(rows, both, both, both, both, rows, rows, both, both, both, both),
        out_specs=(both,) * 6 + (P(None, TP),) * 2,
        check_vma=False,
    )
```

```python
import functools

import jax
import jax.numpy as jnp
from jax import lax
from jax.experimental import pallas as pl
from jax.experimental.pallas import tpu as pltpu
from jax.sharding import Mesh
from jax.sharding import PartitionSpec as P

D = 2048
W = 2048
FS = ("fs_0", "fs_1")
TP = ("tp_0", "tp_1")
NZ, NY, NX, NC = 16, 4, 4, 2
HALF = NZ // 2

first_decay = 0.9
second_decay = 0.9
ratio_floor = 1e-08
mean_floor = 1e-06
step_size = 0.05

f32 = jnp.float32
bf16 = jnp.bfloat16


def remote(src, dst, send_sem, recv_sem, **where):
    return pltpu.make_async_remote_copy(
        src_ref=src,
        dst_ref=dst,
        send_sem=send_sem,
        recv_sem=recv_sem,
        device_id=where,
        device_id_type=pl.DeviceIdType.MESH,
    )


def split_two(v):
    high = v.astype(bf16)
    low = (v - high.astype(f32)).astype(bf16)
    return high, low


def kernel(
    x_hbm, cin_hbm, cg_hbm, min_hbm, mg_hbm, fin_hbm, fg_hbm, a1_hbm, a2_hbm, g1_hbm, g2_hbm,
    step_in, step_g, o_a1, o_a2, o_g1, o_g2, copy_in, copy_g,
    xb, cb, gt, mf, fb, mom, res, lowb, rsy, l2, rsz, rb, dirb, sb, cpy,
    loc_sem, fz_s, fz_r, f1_s, f1_r, f2_s, f2_r, fc_s, fc_r,
    ry_s, ry_r, rz_s, rz_r, gz_s, gz_r, gy_s, gy_r, sc_s, sc_r,
    za_s, za_r, zb_s, zb_r, ya_s, ya_r, yb_s, yb_r, out_sem,
):
    z = lax.axis_index("fs_0")
    y = lax.axis_index("fs_1")
    x = lax.axis_index("tp_0")
    c = lax.axis_index("tp_1")
    other = 1 - c

    def zz(k):
        return lax.rem(z + k + NZ, NZ)

    def yy(k):
        return lax.rem(y + k + NY, NY)

    def xx(k):
        return lax.rem(x + k + NX, NX)

    barrier = pltpu.get_barrier_semaphore()

    def greet(k, _):
        pl.semaphore_signal(barrier, inc=1, device_id={"fs_0": zz(k)}, device_id_type=pl.DeviceIdType.MESH)
        return 0

    near = NZ // 4
    lax.fori_loop(1, near + 1, greet, 0)
    lax.fori_loop(NZ - near, NZ, greet, 0)
    for k in range(1, NY):
        pl.semaphore_signal(barrier, inc=1, device_id={"fs_1": yy(k)}, device_id_type=pl.DeviceIdType.MESH)
    tp_peers = [(dx, dc) for dx in range(NX) for dc in range(NC) if (dx, dc) != (0, 0)]
    for dx, dc in tp_peers:
        pl.semaphore_signal(
            barrier, inc=1,
            device_id={"tp_0": xx(dx), "tp_1": other if dc else c},
            device_id_type=pl.DeviceIdType.MESH,
        )

    h = x // 2
    tile = pl.ds(pl.multiple_of((c * 2 + lax.rem(x, 2)) * 128, 128), 128)
    wide = pl.ds(pl.multiple_of(c * 256, 256), 256)
    piece = pl.ds(pl.multiple_of(lax.rem(x, 2) * 128, 128), 128)

    def own_tile(source):
        return pltpu.make_async_copy(source.at[h, :, piece], fb.at[z, y, h, :, tile], loc_sem.at[0])

    @pl.when(c == 0)
    def _():
        own_tile(fin_hbm).start()

    @pl.when(c == 1)
    def _():
        own_tile(fg_hbm).start()

    loads = [
        pltpu.make_async_copy(min_hbm, mf.at[0, z, y], loc_sem.at[1]),
        pltpu.make_async_copy(mg_hbm, mf.at[1, z, y], loc_sem.at[2]),
        pltpu.make_async_copy(x_hbm, xb, loc_sem.at[3]),
        pltpu.make_async_copy(cin_hbm, cb.at[0], loc_sem.at[4]),
        pltpu.make_async_copy(cg_hbm, cb.at[1], loc_sem.at[5]),
        pltpu.make_async_copy(a1_hbm, mom.at[0], loc_sem.at[6]),
        pltpu.make_async_copy(g1_hbm, mom.at[1], loc_sem.at[7]),
        pltpu.make_async_copy(a2_hbm, mom.at[2], loc_sem.at[8]),
        pltpu.make_async_copy(g2_hbm, mom.at[3], loc_sem.at[9]),
    ]
    for copy in loads:
        copy.start()
    own_tile(fin_hbm).wait()
    for copy in loads[:2]:
        copy.wait()
    pl.semaphore_wait(barrier, 2 * near + NY - 1 + len(tp_peers))

    def step_of(s, way):
        return (zz(1 - s), zz(1)) if way == 0 else (zz(s - 1), zz(-1))

    def za(s, way):
        at, to = step_of(s, way)
        part = mf.at[0, at, y, pl.ds(0, 32) if s < HALF else pl.ds(16 * way, 16)]
        return remote(part, part, za_s.at[way, s], za_r.at[way, s], fs_0=to)

    def zb(s, way):
        at, to = step_of(s, way)
        part = mf.at[1, at, pl.ds(0, 4) if s < HALF else pl.ds(2 * way, 2)]
        return remote(part, part, zb_s.at[way, s], zb_r.at[way, s], fs_0=to)

    def ring_start(make):
        for way in range(2):
            make(1, way).start()

    def ring_next(make, s):
        for way in range(2):
            make(s, way).wait_recv()
            if s < HALF:
                make(s + 1, way).start()

    def ya(o, way):
        part = mf.at[0, zz(o), y]
        return remote(part, part, ya_s.at[way, o], ya_r.at[way, o], fs_1=yy(1 if way == 0 else -1))

    def on(o, way):
        part = mf.at[0, zz(o), yy(-1 if way == 0 else 1), pl.ds(16 * way, 16)]
        return remote(part, part, ya_s.at[way + 2, o], ya_r.at[way + 2, o], fs_1=yy(1 if way == 0 else -1))

    def send_y(offsets):
        for o in offsets:
            for way in range(2):
                ya(o, way).start()

    def pass_y(offsets):
        for o in offsets:
            for way in range(2):
                ya(o, way).wait_recv()
                on(o, way).start()

    yb = [
        remote(mf.at[1, z, y], mf.at[1, z, y], yb_s.at[k], yb_r.at[k], fs_1=yy(k))
        for k in range(1, NY)
    ]

    def fz(k, block=None, to=None):
        part = fb.at[z if block is None else block, y, h, :, tile]
        return remote(part, part, fz_s.at[k], fz_r.at[k], fs_0=zz(k) if to is None else to)

    def relay():
        passed = []
        for j in range(1, near + 1):
            fz(j).wait_recv()
            passed.append(fz(near + j, zz(-j), zz(near)))
            passed[-1].start()
            fz(NZ - j).wait_recv()
            if j < near:
                passed.append(fz(NZ - near - j, zz(j), zz(-near)))
                passed[-1].start()
        return passed

    def start(make):
        def body(k, _):
            make(k).start()
            return 0
        return body

    def wait_recv(make):
        def body(k, _):
            make(k).wait_recv()
            return 0
        return body

    def wait_send(make):
        def body(k, _):
            make(k).wait_send()
            return 0
        return body

    for j in range(1, near + 1):
        fz(j).start()
        fz(NZ - j).start()
    ring_start(za)
    for copy in yb:
        copy.start()
    for copy in loads[2:]:
        copy.wait()

    def gradient(f):
        cot = cb[f].T
        for t in range(4):
            columns = pl.ds(t * 512, 512)
            high, low = split_two(jnp.dot(cot, xb[:, columns], preferred_element_type=f32))
            gt[f, pl.ds(0, 256), columns] = high
            gt[f, pl.ds(256, 256), columns] = low

    gradient(0)
    passed = relay()
    for copy in yb:
        copy.wait_recv()
    ring_start(zb)
    ring_next(za, 1)
    send_y([0, 1, NZ - 1])
    gradient(1)
    ring_next(za, 2)
    send_y([2, NZ - 2])
    ring_next(zb, 1)
    for k in range(near + 1, NZ - near):
        fz(k).wait_recv()

    def half_step(part_x, part_y, send, recv):
        copies = []
        for k in range(1, NX):
            copies.append(remote(part_x, part_x, send.at[0, k], recv.at[0, k], tp_0=xx(k)))
        for k in range(1, NY):
            copies.append(remote(part_y, part_y, send.at[1, k], recv.at[1, k], fs_1=yy(k)))
        for copy in copies:
            copy.start()
        return copies

    lo_z, hi_z = pl.ds(0, HALF), pl.ds(HALF, HALF)
    one = half_step(fb.at[lo_z, y, h, :, tile], fb.at[hi_z, y, h, :, tile], f1_s, f1_r)
    ring_next(za, 3)
    for copy in one:
        copy.wait_recv()
    two = half_step(fb.at[hi_z, :, h, :, tile], fb.at[lo_z, y, :, :, wide], f2_s, f2_r)
    ring_next(zb, 2)
    ring_next(za, 4)
    for copy in two:
        copy.wait_recv()
    mine = fb.at[:, :, :, :, wide]
    swap = remote(mine, mine, fc_s, fc_r, tp_1=other)
    swap.start()
    ring_next(zb, 3)
    pass_y([0, 1, NZ - 1, 2, NZ - 2])
    top = lax.broadcasted_iota(jnp.int32, (32, 8, 128), 1) < 4
    pair = (c, other)

    def project(f):
        factor = fb[:, :, :, :, pl.ds(pl.multiple_of(f * 256, 256), 256)].reshape(D, 256)
        both = jnp.dot(gt[f], factor, preferred_element_type=f32)
        low = (both[:256] + both[256:]).T.reshape(32, 8, 256)
        left, right = low[:, :, :128], low[:, :, 128:]
        even = jnp.where(top, left, pltpu.roll(right, 4, 1)).reshape(16, 2, 8, 128)
        odd = jnp.where(top, pltpu.roll(left, 4, 1), right).reshape(16, 2, 8, 128)
        for k in range(2):
            lowb[f, :, 2 * k] = even[:, k]
            lowb[f, :, 2 * k + 1] = odd[:, k]

    def sum_y(j):
        copies = [
            remote(lowb.at[pair[j], :, yy(k)], rsy.at[j, k - 1], ry_s.at[j, k], ry_r.at[j, k], fs_1=yy(k))
            for k in range(1, NY)
        ]
        for copy in copies:
            copy.start()
        return copies

    def rz(j):
        return lambda k: remote(l2.at[j, zz(k)], rsz.at[j, k], rz_s.at[j, k], rz_r.at[j, k], fs_0=zz(k))

    def gz(j):
        part = rb.at[j, z, y]
        return lambda k: remote(part, part, gz_s.at[j, k], gz_r.at[j, k], fs_0=zz(k))

    project(c)
    ry = [sum_y(0)]
    ring_next(za, 5)
    swap.wait_recv()
    project(other)
    ry.append(sum_y(1))
    ring_next(zb, 4)
    ring_next(za, 6)
    for j in range(2):
        acc = lowb[pair[j], :, y]
        for k, copy in enumerate(ry[j]):
            copy.wait_recv()
            acc = acc + rsy[j, k]
        l2[j] = acc
        lax.fori_loop(1, NZ, start(rz(j)), 0)
    early = [o for s in range(3, HALF - 1) for o in (s, NZ - s)]
    late = [HALF - 1, HALF + 1, HALF]
    send_y(early)
    ring_next(zb, 5)

    def folded(v):
        return jnp.concatenate([v[:, :128], v[:, 128:]], axis=0)

    def unfolded(v):
        return jnp.concatenate([v[:4], v[4:]], axis=1)

    for j in range(2):
        def add_one(k, total, j=j):
            rz(j)(k).wait_recv()
            return total + rsz[j, k]

        low = lax.fori_loop(1, NZ, add_one, l2[j, z])
        first_new = first_decay * folded(mom[pair[j]]) + (1.0 - first_decay) * low
        second_new = second_decay * folded(mom[2 + pair[j]]) + (1.0 - second_decay) * low * low
        rb[j, z, y] = first_new / (jnp.sqrt(second_new) + ratio_floor)
        lax.fori_loop(1, NZ, start(gz(j)), 0)
        res[pair[j]] = unfolded(first_new)
        res[2 + pair[j]] = unfolded(second_new)
    pass_y(early)
    gy = []
    for j in range(2):
        lax.fori_loop(1, NZ, wait_recv(gz(j)), 0)
        part = rb.at[j, :, y]
        gy.append([
            remote(part, part, gy_s.at[j, k], gy_r.at[j, k], fs_1=yy(k)) for k in range(1, NY)
        ])
        for copy in gy[j]:
            copy.start()
    for k, out in enumerate((o_a1, o_g1, o_a2, o_g2)):
        out[...] = res[k]
    ring_next(zb, 6)
    ring_next(za, 7)
    ring_next(za, HALF)
    send_y(late)
    ring_next(zb, 7)
    for j in range(2):
        f = pair[j]
        for copy in gy[j]:
            copy.wait_recv()
        ratio = rb[j].reshape(32, 2, 8, 128)
        even, odd = ratio[:, 0], ratio[:, 1]
        left = jnp.where(top, even, pltpu.roll(odd, 4, 1)).reshape(256, 128)
        right = jnp.where(top, pltpu.roll(even, 4, 1), odd).reshape(256, 128)
        high, lo = split_two(jnp.concatenate([left, right], axis=1))
        acc = jnp.zeros((8, 256), f32)
        for t in range(4):
            block = fb[4 * t:4 * t + 4, :, :, :, pl.ds(pl.multiple_of(f * 256, 256), 256)].reshape(512, 256)
            d = jnp.dot(block, high, preferred_element_type=f32)
            d = d + jnp.dot(block, lo, preferred_element_type=f32)
            dirb[f, t] = d.reshape(16, 32, 256)
            acc = acc + jnp.sum((d * d).reshape(64, 8, 256), axis=0)
        sb[0, f] = acc[:, :128] + acc[:, 128:]

    sc = [
        remote(
            sb.at[0], sb.at[k + 1], sc_s.at[k], sc_r.at[k],
            tp_0=xx(dx), tp_1=other if dc else c,
        )
        for k, (dx, dc) in enumerate(tp_peers)
    ]
    for copy in sc:
        copy.start()
    pass_y(late)
    ring_next(zb, HALF)
    for o in range(NZ):
        for way in range(2):
            on(o, way).wait_recv()
    for copy in sc:
        copy.wait_recv()
    outs = []
    for f, (out, whole) in enumerate(((step_in, copy_in), (step_g, copy_g))):
        total = jnp.sum(jnp.sum(sb[:, f], axis=0), keepdims=True)
        scale = lax.rsqrt(total / (D * W) + mean_floor)
        for t in range(4):
            step = dirb[f, t] * scale.reshape(1, 1, 1)
            weights = mf[f, 4 * t:4 * t + 4].reshape(16, 32, 256)
            cpy[f, t] = (weights - step_size * step).astype(bf16)
            outs.append(pltpu.make_async_copy(cpy.at[f, t], whole.at[t], out_sem.at[f, t]))
            outs[-1].start()
        out[...] = dirb[f, z // 4, lax.rem(z, 4) * NY + y] * scale

    for k in range(1, NZ):
        fz(k).wait_send()
    for j in range(2):
        lax.fori_loop(1, NZ, wait_send(rz(j)), 0)
        lax.fori_loop(1, NZ, wait_send(gz(j)), 0)
    for copy in [*one, *two, swap, *ry[0], *ry[1], *gy[0], *gy[1], *sc, *yb]:
        copy.wait_send()
    for way in range(2):
        for s in range(1, HALF + 1):
            za(s, way).wait_send()
            zb(s, way).wait_send()
        for o in range(NZ):
            ya(o, way).wait_send()
            on(o, way).wait_send()
    for copy in outs:
        copy.wait()


def deliver(*refs):
    sem = refs[16]
    copies = [pltpu.make_async_copy(refs[i], refs[8 + i], sem.at[i]) for i in range(8)]
    for copy in copies:
        copy.start()
    for copy in copies:
        copy.wait()


def local(*args):
    vmem = pl.BlockSpec(memory_space=pltpu.VMEM)
    anywhere = pl.BlockSpec(memory_space=pl.ANY)
    dma = pltpu.SemaphoreType.DMA
    args = list(args)
    for k in (5, 6):
        args[k] = args[k].reshape(2, 16, 256)
    shapes = [jax.ShapeDtypeStruct((32, 256), f32)] * 2 + [jax.ShapeDtypeStruct((4, 256), f32)] * 4
    shapes += [jax.ShapeDtypeStruct((4, 16, 32, 256), bf16)] * 2
    out = pl.pallas_call(
        kernel,
        out_shape=tuple(shapes),
        in_specs=[anywhere] * 11,
        out_specs=(vmem,) * 6 + (anywhere,) * 2,
        scratch_shapes=[
            pltpu.VMEM((768, 2048), bf16),
            pltpu.VMEM((2, 768, 256), bf16),
            pltpu.VMEM((2, 512, 2048), bf16),
            pltpu.VMEM((2, NZ, NY, 32, 256), f32),
            pltpu.VMEM((NZ, NY, 2, 16, 512), bf16),
            pltpu.VMEM((4, 4, 256), f32),
            pltpu.VMEM((4, 4, 256), f32),
            pltpu.VMEM((2, NZ, NY, 8, 128), f32),
            pltpu.VMEM((2, NY - 1, NZ, 8, 128), f32),
            pltpu.VMEM((2, NZ, 8, 128), f32),
            pltpu.VMEM((2, NZ, 8, 128), f32),
            pltpu.VMEM((2, NZ, NY, 8, 128), f32),
            pltpu.VMEM((2, 4, 16, 32, 256), f32),
            pltpu.VMEM((NX * NC, 2, 8, 128), f32),
            pltpu.VMEM((2, 4, 16, 32, 256), bf16),
            dma((10,)),
            dma((NZ,)), dma((NZ,)),
            dma((2, 4)), dma((2, 4)), dma((2, 4)), dma((2, 4)),
            dma, dma,
            dma((2, NY)), dma((2, NY)), dma((2, NZ)), dma((2, NZ)),
            dma((2, NZ)), dma((2, NZ)), dma((2, NY)), dma((2, NY)),
            dma((NX * NC,)), dma((NX * NC,)),
            dma((2, HALF + 1)), dma((2, HALF + 1)), dma((2, HALF + 1)), dma((2, HALF + 1)),
            dma((4, NZ)), dma((4, NZ)), dma((NY,)), dma((NY,)),
            dma((2, 4)),
        ],
        compiler_params=pltpu.CompilerParams(
            collective_id=0, has_side_effects=True, vmem_limit_bytes=40 * 1024 * 1024
        ),
    )(*[pltpu.with_memory_space_constraint(a, pltpu.HBM) for a in args])
    out = pl.pallas_call(
        deliver,
        out_shape=tuple(shapes),
        in_specs=[anywhere] * 8,
        out_specs=(anywhere,) * 8,
        scratch_shapes=[dma((8,))],
        compiler_params=pltpu.CompilerParams(vmem_limit_bytes=1024 * 1024),
    )(*out)
    return (*out[:6], out[6].reshape(D, 256), out[7].reshape(D, 256))


def solution(mesh):
    finer = Mesh(mesh.devices.reshape(NZ, NY, NX, NC), ("fs_0", "fs_1", "tp_0", "tp_1"))
    rows, both = P(FS, None), P(FS, TP)
    return jax.shard_map(
        local,
        mesh=finer,
        in_specs=(rows, both, both, both, both, rows, rows, both, both, both, both),
        out_specs=(both,) * 6 + (P(None, TP),) * 2,
        check_vma=False,
    )
```

```python
import functools

import jax
import jax.numpy as jnp
from jax import lax
from jax.experimental import pallas as pl
from jax.experimental.pallas import tpu as pltpu
from jax.sharding import Mesh
from jax.sharding import PartitionSpec as P

D = 2048
W = 2048
FS = ("fs_0", "fs_1")
TP = ("tp_0", "tp_1")
NZ, NY, NX, NC = 16, 4, 4, 2
HALF = NZ // 2

first_decay = 0.9
second_decay = 0.9
ratio_floor = 1e-08
mean_floor = 1e-06
step_size = 0.05

f32 = jnp.float32
bf16 = jnp.bfloat16


def remote(src, dst, send_sem, recv_sem, **where):
    return pltpu.make_async_remote_copy(
        src_ref=src,
        dst_ref=dst,
        send_sem=send_sem,
        recv_sem=recv_sem,
        device_id=where,
        device_id_type=pl.DeviceIdType.MESH,
    )


def split_two(v):
    high = v.astype(bf16)
    low = (v - high.astype(f32)).astype(bf16)
    return high, low


def kernel(
    x_hbm, cin_hbm, cg_hbm, min_hbm, mg_hbm, fin_hbm, fg_hbm, a1_hbm, a2_hbm, g1_hbm, g2_hbm,
    step_in, step_g, o_a1, o_a2, o_g1, o_g2, copy_in, copy_g,
    xb, cb, gt, mf, fb, mom, res, lowb, rsy, l2, rsz, rb, dirb, sb, cpy,
    loc_sem, fz_s, fz_r, f1_s, f1_r, f2_s, f2_r, fc_s, fc_r,
    ry_s, ry_r, rz_s, rz_r, gz_s, gz_r, gy_s, gy_r, sc_s, sc_r,
    za_s, za_r, zb_s, zb_r, ya_s, ya_r, yb_s, yb_r, out_sem,
):
    z = lax.axis_index("fs_0")
    y = lax.axis_index("fs_1")
    x = lax.axis_index("tp_0")
    c = lax.axis_index("tp_1")
    other = 1 - c

    def zz(k):
        return lax.rem(z + k + NZ, NZ)

    def yy(k):
        return lax.rem(y + k + NY, NY)

    def xx(k):
        return lax.rem(x + k + NX, NX)

    barrier = pltpu.get_barrier_semaphore()

    def greet(k, _):
        pl.semaphore_signal(barrier, inc=1, device_id={"fs_0": zz(k)}, device_id_type=pl.DeviceIdType.MESH)
        return 0

    near = NZ // 4
    lax.fori_loop(1, near + 1, greet, 0)
    lax.fori_loop(NZ - near, NZ, greet, 0)
    for k in range(1, NY):
        pl.semaphore_signal(barrier, inc=1, device_id={"fs_1": yy(k)}, device_id_type=pl.DeviceIdType.MESH)
    tp_peers = [(dx, dc) for dx in range(NX) for dc in range(NC) if (dx, dc) != (0, 0)]
    for dx, dc in tp_peers:
        pl.semaphore_signal(
            barrier, inc=1,
            device_id={"tp_0": xx(dx), "tp_1": other if dc else c},
            device_id_type=pl.DeviceIdType.MESH,
        )

    h = x // 2
    tile = pl.ds(pl.multiple_of((c * 2 + lax.rem(x, 2)) * 128, 128), 128)
    wide = pl.ds(pl.multiple_of(c * 256, 256), 256)
    piece = pl.ds(pl.multiple_of(lax.rem(x, 2) * 128, 128), 128)

    def own_tile(source):
        return pltpu.make_async_copy(source.at[h, :, piece], fb.at[z, y, h, :, tile], loc_sem.at[0])

    @pl.when(c == 0)
    def _():
        own_tile(fin_hbm).start()

    @pl.when(c == 1)
    def _():
        own_tile(fg_hbm).start()

    loads = [
        pltpu.make_async_copy(min_hbm, mf.at[0, z, y], loc_sem.at[1]),
        pltpu.make_async_copy(mg_hbm, mf.at[1, z, y], loc_sem.at[2]),
        pltpu.make_async_copy(x_hbm, xb, loc_sem.at[3]),
        pltpu.make_async_copy(cin_hbm, cb.at[0], loc_sem.at[4]),
        pltpu.make_async_copy(cg_hbm, cb.at[1], loc_sem.at[5]),
        pltpu.make_async_copy(a1_hbm, mom.at[0], loc_sem.at[6]),
        pltpu.make_async_copy(g1_hbm, mom.at[1], loc_sem.at[7]),
        pltpu.make_async_copy(a2_hbm, mom.at[2], loc_sem.at[8]),
        pltpu.make_async_copy(g2_hbm, mom.at[3], loc_sem.at[9]),
    ]
    for copy in loads:
        copy.start()
    own_tile(fin_hbm).wait()
    for copy in loads[:2]:
        copy.wait()
    pl.semaphore_wait(barrier, 2 * near + NY - 1 + len(tp_peers))

    def step_of(s, way):
        return (zz(1 - s), zz(1)) if way == 0 else (zz(s - 1), zz(-1))

    def za(s, way):
        at, to = step_of(s, way)
        part = mf.at[0, at, y, pl.ds(0, 32) if s < HALF else pl.ds(16 * way, 16)]
        return remote(part, part, za_s.at[way, s], za_r.at[way, s], fs_0=to)

    def zb(s, way):
        at, to = step_of(s, way)
        part = mf.at[1, at, pl.ds(0, 4) if s < HALF else pl.ds(2 * way, 2)]
        return remote(part, part, zb_s.at[way, s], zb_r.at[way, s], fs_0=to)

    def ring_start(make):
        for way in range(2):
            make(1, way).start()

    def ring_next(make, s):
        for way in range(2):
            make(s, way).wait_recv()
            if s < HALF:
                make(s + 1, way).start()

    def ya(o, way):
        part = mf.at[0, zz(o), y]
        return remote(part, part, ya_s.at[way, o], ya_r.at[way, o], fs_1=yy(1 if way == 0 else -1))

    def on(o, way):
        part = mf.at[0, zz(o), yy(-1 if way == 0 else 1), pl.ds(16 * way, 16)]
        return remote(part, part, ya_s.at[way + 2, o], ya_r.at[way + 2, o], fs_1=yy(1 if way == 0 else -1))

    def send_y(offsets):
        for o in offsets:
            for way in range(2):
                ya(o, way).start()

    def pass_y(offsets):
        for o in offsets:
            for way in range(2):
                ya(o, way).wait_recv()
                on(o, way).start()

    yb = [
        remote(mf.at[1, z, y], mf.at[1, z, y], yb_s.at[k], yb_r.at[k], fs_1=yy(k))
        for k in range(1, NY)
    ]

    def fz(k, block=None, to=None):
        part = fb.at[z if block is None else block, y, h, :, tile]
        return remote(part, part, fz_s.at[k], fz_r.at[k], fs_0=zz(k) if to is None else to)

    def relay():
        passed = []
        for j in range(1, near + 1):
            fz(j).wait_recv()
            passed.append(fz(near + j, zz(-j), zz(near)))
            passed[-1].start()
            fz(NZ - j).wait_recv()
            if j < near:
                passed.append(fz(NZ - near - j, zz(j), zz(-near)))
                passed[-1].start()
        return passed

    def start(make):
        def body(k, _):
            make(k).start()
            return 0
        return body

    def wait_recv(make):
        def body(k, _):
            make(k).wait_recv()
            return 0
        return body

    def wait_send(make):
        def body(k, _):
            make(k).wait_send()
            return 0
        return body

    for j in range(1, near + 1):
        fz(j).start()
        fz(NZ - j).start()
    ring_start(za)
    for copy in yb:
        copy.start()
    for copy in loads[2:]:
        copy.wait()

    def gradient(f):
        cot = cb[f].T
        for t in range(4):
            columns = pl.ds(t * 512, 512)
            high, low = split_two(jnp.dot(cot, xb[:, columns], preferred_element_type=f32))
            gt[f, pl.ds(0, 256), columns] = high
            gt[f, pl.ds(256, 256), columns] = low

    passed = relay()
    for copy in yb:
        copy.wait_recv()
    ring_start(zb)
    ring_next(za, 1)
    send_y([0, 1, NZ - 1])
    ring_next(za, 2)
    send_y([2, NZ - 2])
    ring_next(zb, 1)
    for k in range(near + 1, NZ - near):
        fz(k).wait_recv()

    def half_step(part_x, part_y, send, recv):
        copies = []
        for k in range(1, NX):
            copies.append(remote(part_x, part_x, send.at[0, k], recv.at[0, k], tp_0=xx(k)))
        for k in range(1, NY):
            copies.append(remote(part_y, part_y, send.at[1, k], recv.at[1, k], fs_1=yy(k)))
        for copy in copies:
            copy.start()
        return copies

    lo_z, hi_z = pl.ds(0, HALF), pl.ds(HALF, HALF)
    one = half_step(fb.at[lo_z, y, h, :, tile], fb.at[hi_z, y, h, :, tile], f1_s, f1_r)
    ring_next(za, 3)
    for copy in one:
        copy.wait_recv()
    two = half_step(fb.at[hi_z, :, h, :, tile], fb.at[lo_z, y, :, :, wide], f2_s, f2_r)
    gradient(0)
    ring_next(zb, 2)
    gradient(1)
    ring_next(za, 4)
    for copy in two:
        copy.wait_recv()
    mine = fb.at[:, :, :, :, wide]
    swap = remote(mine, mine, fc_s, fc_r, tp_1=other)
    swap.start()
    ring_next(zb, 3)
    pass_y([0, 1, NZ - 1, 2, NZ - 2])
    top = lax.broadcasted_iota(jnp.int32, (32, 8, 128), 1) < 4
    pair = (c, other)

    def project(f):
        factor = fb[:, :, :, :, pl.ds(pl.multiple_of(f * 256, 256), 256)].reshape(D, 256)
        both = jnp.dot(gt[f], factor, preferred_element_type=f32)
        low = (both[:256] + both[256:]).T.reshape(32, 8, 256)
        left, right = low[:, :, :128], low[:, :, 128:]
        even = jnp.where(top, left, pltpu.roll(right, 4, 1)).reshape(16, 2, 8, 128)
        odd = jnp.where(top, pltpu.roll(left, 4, 1), right).reshape(16, 2, 8, 128)
        for k in range(2):
            lowb[f, :, 2 * k] = even[:, k]
            lowb[f, :, 2 * k + 1] = odd[:, k]

    def sum_y(j):
        copies = [
            remote(lowb.at[pair[j], :, yy(k)], rsy.at[j, k - 1], ry_s.at[j, k], ry_r.at[j, k], fs_1=yy(k))
            for k in range(1, NY)
        ]
        for copy in copies:
            copy.start()
        return copies

    def rz(j):
        return lambda k: remote(l2.at[j, zz(k)], rsz.at[j, k], rz_s.at[j, k], rz_r.at[j, k], fs_0=zz(k))

    def gz(j):
        part = rb.at[j, z, y]
        return lambda k: remote(part, part, gz_s.at[j, k], gz_r.at[j, k], fs_0=zz(k))

    project(c)
    ry = [sum_y(0)]
    ring_next(za, 5)
    swap.wait_recv()
    project(other)
    ry.append(sum_y(1))
    ring_next(zb, 4)
    ring_next(za, 6)
    for j in range(2):
        acc = lowb[pair[j], :, y]
        for k, copy in enumerate(ry[j]):
            copy.wait_recv()
            acc = acc + rsy[j, k]
        l2[j] = acc
        lax.fori_loop(1, NZ, start(rz(j)), 0)
    early = [o for s in range(3, HALF - 1) for o in (s, NZ - s)]
    late = [HALF - 1, HALF + 1, HALF]
    send_y(early)
    ring_next(zb, 5)

    def folded(v):
        return jnp.concatenate([v[:, :128], v[:, 128:]], axis=0)

    def unfolded(v):
        return jnp.concatenate([v[:4], v[4:]], axis=1)

    for j in range(2):
        def add_one(k, total, j=j):
            rz(j)(k).wait_recv()
            return total + rsz[j, k]

        low = lax.fori_loop(1, NZ, add_one, l2[j, z])
        first_new = first_decay * folded(mom[pair[j]]) + (1.0 - first_decay) * low
        second_new = second_decay * folded(mom[2 + pair[j]]) + (1.0 - second_decay) * low * low
        rb[j, z, y] = first_new / (jnp.sqrt(second_new) + ratio_floor)
        lax.fori_loop(1, NZ, start(gz(j)), 0)
        res[pair[j]] = unfolded(first_new)
        res[2 + pair[j]] = unfolded(second_new)
    pass_y(early)
    gy = []
    for j in range(2):
        lax.fori_loop(1, NZ, wait_recv(gz(j)), 0)
        part = rb.at[j, :, y]
        gy.append([
            remote(part, part, gy_s.at[j, k], gy_r.at[j, k], fs_1=yy(k)) for k in range(1, NY)
        ])
        for copy in gy[j]:
            copy.start()
    for k, out in enumerate((o_a1, o_g1, o_a2, o_g2)):
        out[...] = res[k]
    ring_next(zb, 6)
    ring_next(za, 7)
    ring_next(za, HALF)
    send_y(late)
    for j in range(2):
        f = pair[j]
        for copy in gy[j]:
            copy.wait_recv()
        ratio = rb[j].reshape(32, 2, 8, 128)
        even, odd = ratio[:, 0], ratio[:, 1]
        left = jnp.where(top, even, pltpu.roll(odd, 4, 1)).reshape(256, 128)
        right = jnp.where(top, pltpu.roll(even, 4, 1), odd).reshape(256, 128)
        high, lo = split_two(jnp.concatenate([left, right], axis=1))
        acc = jnp.zeros((8, 256), f32)
        for t in range(4):
            block = fb[4 * t:4 * t + 4, :, :, :, pl.ds(pl.multiple_of(f * 256, 256), 256)].reshape(512, 256)
            d = jnp.dot(block, high, preferred_element_type=f32)
            d = d + jnp.dot(block, lo, preferred_element_type=f32)
            dirb[f, t] = d.reshape(16, 32, 256)
            acc = acc + jnp.sum((d * d).reshape(64, 8, 256), axis=0)
        sb[0, f] = acc[:, :128] + acc[:, 128:]

    sc = [
        remote(
            sb.at[0], sb.at[k + 1], sc_s.at[k], sc_r.at[k],
            tp_0=xx(dx), tp_1=other if dc else c,
        )
        for k, (dx, dc) in enumerate(tp_peers)
    ]
    for copy in sc:
        copy.start()
    ring_next(zb, 7)
    pass_y(late)
    ring_next(zb, HALF)
    for o in range(NZ):
        for way in range(2):
            on(o, way).wait_recv()
    for copy in sc:
        copy.wait_recv()
    outs = []
    for f, (out, whole) in enumerate(((step_in, copy_in), (step_g, copy_g))):
        total = jnp.sum(jnp.sum(sb[:, f], axis=0), keepdims=True)
        scale = lax.rsqrt(total / (D * W) + mean_floor)
        for t in range(4):
            step = dirb[f, t] * scale.reshape(1, 1, 1)
            weights = mf[f, 4 * t:4 * t + 4].reshape(16, 32, 256)
            cpy[f, t] = (weights - step_size * step).astype(bf16)
            outs.append(pltpu.make_async_copy(cpy.at[f, t], whole.at[t], out_sem.at[f, t]))
            outs[-1].start()
        out[...] = dirb[f, z // 4, lax.rem(z, 4) * NY + y] * scale

    for k in range(1, NZ):
        fz(k).wait_send()
    for j in range(2):
        lax.fori_loop(1, NZ, wait_send(rz(j)), 0)
        lax.fori_loop(1, NZ, wait_send(gz(j)), 0)
    for copy in [*one, *two, swap, *ry[0], *ry[1], *gy[0], *gy[1], *sc, *yb]:
        copy.wait_send()
    for way in range(2):
        for s in range(1, HALF + 1):
            za(s, way).wait_send()
            zb(s, way).wait_send()
        for o in range(NZ):
            ya(o, way).wait_send()
            on(o, way).wait_send()
    for copy in outs:
        copy.wait()


def deliver(*refs):
    sem = refs[16]
    copies = [pltpu.make_async_copy(refs[i], refs[8 + i], sem.at[i]) for i in range(8)]
    for copy in copies:
        copy.start()
    for copy in copies:
        copy.wait()


def local(*args):
    vmem = pl.BlockSpec(memory_space=pltpu.VMEM)
    anywhere = pl.BlockSpec(memory_space=pl.ANY)
    dma = pltpu.SemaphoreType.DMA
    args = list(args)
    for k in (5, 6):
        args[k] = args[k].reshape(2, 16, 256)
    shapes = [jax.ShapeDtypeStruct((32, 256), f32)] * 2 + [jax.ShapeDtypeStruct((4, 256), f32)] * 4
    shapes += [jax.ShapeDtypeStruct((4, 16, 32, 256), bf16)] * 2
    out = pl.pallas_call(
        kernel,
        out_shape=tuple(shapes),
        in_specs=[anywhere] * 11,
        out_specs=(vmem,) * 6 + (anywhere,) * 2,
        scratch_shapes=[
            pltpu.VMEM((768, 2048), bf16),
            pltpu.VMEM((2, 768, 256), bf16),
            pltpu.VMEM((2, 512, 2048), bf16),
            pltpu.VMEM((2, NZ, NY, 32, 256), f32),
            pltpu.VMEM((NZ, NY, 2, 16, 512), bf16),
            pltpu.VMEM((4, 4, 256), f32),
            pltpu.VMEM((4, 4, 256), f32),
            pltpu.VMEM((2, NZ, NY, 8, 128), f32),
            pltpu.VMEM((2, NY - 1, NZ, 8, 128), f32),
            pltpu.VMEM((2, NZ, 8, 128), f32),
            pltpu.VMEM((2, NZ, 8, 128), f32),
            pltpu.VMEM((2, NZ, NY, 8, 128), f32),
            pltpu.VMEM((2, 4, 16, 32, 256), f32),
            pltpu.VMEM((NX * NC, 2, 8, 128), f32),
            pltpu.VMEM((2, 4, 16, 32, 256), bf16),
            dma((10,)),
            dma((NZ,)), dma((NZ,)),
            dma((2, 4)), dma((2, 4)), dma((2, 4)), dma((2, 4)),
            dma, dma,
            dma((2, NY)), dma((2, NY)), dma((2, NZ)), dma((2, NZ)),
            dma((2, NZ)), dma((2, NZ)), dma((2, NY)), dma((2, NY)),
            dma((NX * NC,)), dma((NX * NC,)),
            dma((2, HALF + 1)), dma((2, HALF + 1)), dma((2, HALF + 1)), dma((2, HALF + 1)),
            dma((4, NZ)), dma((4, NZ)), dma((NY,)), dma((NY,)),
            dma((2, 4)),
        ],
        compiler_params=pltpu.CompilerParams(
            collective_id=0, has_side_effects=True, vmem_limit_bytes=40 * 1024 * 1024
        ),
    )(*[pltpu.with_memory_space_constraint(a, pltpu.HBM) for a in args])
    out = pl.pallas_call(
        deliver,
        out_shape=tuple(shapes),
        in_specs=[anywhere] * 8,
        out_specs=(anywhere,) * 8,
        scratch_shapes=[dma((8,))],
        compiler_params=pltpu.CompilerParams(vmem_limit_bytes=1024 * 1024),
    )(*out)
    return (*out[:6], out[6].reshape(D, 256), out[7].reshape(D, 256))


def solution(mesh):
    finer = Mesh(mesh.devices.reshape(NZ, NY, NX, NC), ("fs_0", "fs_1", "tp_0", "tp_1"))
    rows, both = P(FS, None), P(FS, TP)
    return jax.shard_map(
        local,
        mesh=finer,
        in_specs=(rows, both, both, both, both, rows, rows, both, both, both, both),
        out_specs=(both,) * 6 + (P(None, TP),) * 2,
        check_vma=False,
    )
```
